256 devices in a mesh: sp: 64 (over z, y, core), tp: 4 (over x).
Axes of the slice: x: 4, y: 4, z: 8, core: 2. Of those that a mesh axis runs over, the one named last changes fastest.
Arguments:
- queries: bfloat16 [32768, 1024], P('sp', 'tp'), may hold values from -60 to 60
- keys: bfloat16 [32768, 1024], P('sp', 'tp'), may hold values from -6 to 6
- values: bfloat16 [32768, 1024], P('sp', 'tp'), may hold values from -6 to 6
- lambdas: float32 [8], P('tp'), may hold values from 0.3 to 0.8
- head_gain: float32 [128], replicated, may hold values from 0.1 to 1.9
- w_out: bfloat16 [1024, 2048], replicated, may hold values from -0.1875 to 0.1875
- residual_in: bfloat16 [32768, 2048], P(('sp', 'tp')), may hold values from -6 to 6
- norm_gain: float32 [2048], replicated, may hold values from 0.1 to 1.9
- route_ids: int32 [32768, 2], P(('sp', 'tp')), may hold values from 0 to 63, as said below
- route_weight: float32 [32768, 2], P(('sp', 'tp')), may hold values from 0.2 to 1
- w_gate: bfloat16 [64, 2048, 1024], P('sp', None, 'tp'), may hold values from -0.125 to 0.125
- w_up: bfloat16 [64, 2048, 1024], P('sp', None, 'tp'), may hold values from -0.125 to 0.125
- w_down: bfloat16 [64, 2048, 1024], P('sp', None, 'tp'), may hold values from -0.1875 to 0.1875
Outputs:
- layer_out: bfloat16 [32768, 2048], P(('sp', 'tp'))
The draws below stay inside these ranges and needn't reach their ends.
Inputs may be any that keep to these rules, and one draw needn't show every extreme that they name: `route_ids`: each row names two different experts of one group (the same expert // 8). Among the 128 rows of one device (aligned blocks), no expert is named more than 8 times, and in every draw one expert is named exactly 8 times in the rows of every device.
All inputs are finite; a program needn't handle non-finite values.
Results may differ from the reference program's by a relative error of at most 0.015.
Values may be sent and summed in bfloat16 or wider, within the bound.
A program may use at most 128 MiB of HBM per device.

```python
import jax
import jax.numpy as jnp
from jax import lax

D = 2048
HEADS = 8
HEAD_DIM = 64
FF = 1024
GROUP_SIZE = 8
SEQ_LEN = 8192
SEQUENCES = 4
TOKENS = 32768
DEV_ROWS = 128
EXPERTS = 64
GROUPS = 8
CAPACITY = 8


def base_field(key, salt_value):
    array_shape = (TOKENS, HEADS * 2 * HEAD_DIM)
    subkey = jax.random.fold_in(key, salt_value)
    return jnp.clip(1.3 * jax.random.normal(subkey, array_shape, jnp.float32), -5.5, 5.5)


def draw_keys(key, part):
    base_values = base_field(key, 11)
    return base_values.astype(jnp.bfloat16)


def draw_queries(key, part):
    base_values = base_field(key, 12)
    return base_values.astype(jnp.bfloat16)


def draw_route_ids(key, part):
    block_count = TOKENS // DEV_ROWS
    pair_count = EXPERTS * CAPACITY // 2
    favored = jax.random.randint(jax.random.fold_in(key, 31), (), 0, EXPERTS)
    round_offsets = (jnp.arange(GROUPS * CAPACITY, dtype=jnp.int32) // CAPACITY)[:, None] * GROUP_SIZE

    def one_block(block_key):
        round_keys = jax.random.split(jax.random.fold_in(block_key, 1), GROUPS * CAPACITY)
        rounds = jax.vmap(lambda round_key: jax.random.permutation(round_key, GROUP_SIZE))(round_keys)
        pair_table = (rounds.astype(jnp.int32) + round_offsets).reshape(pair_count, 2)
        holds_favored = jnp.any(pair_table == favored, axis=1).astype(jnp.int32)
        jitter_values = jax.random.randint(jax.random.fold_in(block_key, 2), (pair_count,), 0, 1 << 18)
        priority = (jitter_values + holds_favored * (1 << 18)) * pair_count + jnp.arange(pair_count, dtype=jnp.int32)
        unused, picked = lax.top_k(priority, DEV_ROWS)
        shuffle = jax.random.permutation(jax.random.fold_in(block_key, 3), DEV_ROWS)
        return pair_table[picked][shuffle]
    block_keys = jax.vmap(lambda block_index: jax.random.fold_in(jax.random.fold_in(key, 32), block_index))(jnp.arange(block_count))
    return jax.vmap(one_block)(block_keys).reshape(TOKENS, 2).astype(jnp.int32)


def steps_of(own_key, shape, shards, low, largest):
    level = 1.0
    for position, parts in shards:
        steps = jax.random.uniform(jax.random.fold_in(jax.random.fold_in(own_key, 6), position), (parts,), jnp.float32, low / len(shards), largest / len(shards))
        level = level * jnp.repeat(jnp.exp(steps), shape[position] // parts).reshape((-1,) + (1,) * (len(shape) - 1 - position))
    return level


def scatter_about(stream_key, shape, deviation, reach, shards=(), held_as=jnp.bfloat16):
    drawn = deviation * jax.random.normal(stream_key, shape, jnp.float32)
    if shards:
        drawn = drawn * steps_of(stream_key, shape, shards, -0.22, 0.18)
    return jnp.clip(drawn, -reach, reach).astype(held_as)


def setup_inputs(seed: int = 0) -> dict:
    splits = jax.random.split(jax.random.key(seed), 14)
    queries = draw_queries(jax.random.fold_in(splits[13], 71), 0)
    keys = draw_keys(jax.random.fold_in(splits[13], 71), 0)
    values = scatter_about(splits[2], (TOKENS, HEADS * 2 * HEAD_DIM), 1.0, 6.0, ((0, 64), (1, 4)))
    lambdas = jnp.clip(0.3 + 0.5 * jax.random.uniform(splits[3], (HEADS,), jnp.float32) ** steps_of(splits[3], (HEADS,), ((0, 4),), -0.2, 0.2), 0.3, 0.8)
    head_gain = jnp.clip(1.0 + 0.18 * jax.random.normal(splits[4], (2 * HEAD_DIM,), jnp.float32), 0.1, 1.9)
    w_out = scatter_about(splits[5], (HEADS * 2 * HEAD_DIM, D), (HEADS * 2 * HEAD_DIM) ** -0.5, 0.1875)
    residual_in = scatter_about(splits[6], (TOKENS, D), 1.0, 6.0, ((0, 256),))
    norm_gain = jnp.clip(1.0 + 0.18 * jax.random.normal(splits[7], (D,), jnp.float32), 0.1, 1.9)
    route_ids = draw_route_ids(jax.random.fold_in(splits[13], 71), 0)
    route_weight = jnp.clip(0.2 + 0.8 * jax.random.uniform(splits[9], (TOKENS, 2), jnp.float32) ** steps_of(splits[9], (TOKENS, 2), ((0, 256),), -0.2, 0.2), 0.2, 1.0)
    w_gate = scatter_about(splits[10], (EXPERTS, D, FF), D ** -0.5, 0.125, ((0, 64), (2, 4)))
    w_up = scatter_about(splits[11], (EXPERTS, D, FF), D ** -0.5, 0.125, ((0, 64), (2, 4)))
    w_down = scatter_about(splits[12], (EXPERTS, D, FF), FF ** -0.5, 0.1875, ((0, 64), (2, 4)))
    return {"queries": queries, "keys": keys, "values": values, "lambdas": lambdas, "head_gain": head_gain, "w_out": w_out, "residual_in": residual_in, "norm_gain": norm_gain, "route_ids": route_ids, "route_weight": route_weight, "w_gate": w_gate, "w_up": w_up, "w_down": w_down}


EPSILON = 1e-06
OUT_SCALE = 0.8

def slot_numbers(flat_ids):
    count_ids = flat_ids.shape[0]
    positions = lax.broadcasted_iota(jnp.int32, (count_ids, count_ids), 0)
    earlier = lax.broadcasted_iota(jnp.int32, (count_ids, count_ids), 1) < positions
    matches = (flat_ids[:, None] == flat_ids[None, :]) & earlier
    return lax.optimization_barrier(jnp.sum(matches.astype(jnp.int32), axis=1))

def attend_block(query_block, key_view, value_view, lambdas, head_gain):
    scores = jnp.einsum('qhmd,khmd->hmqk', query_block.astype(jnp.float32), key_view) * HEAD_DIM ** (-0.5)
    peak_score = lax.optimization_barrier(jnp.max(scores, axis=-1, keepdims=True))
    weights = jnp.exp(scores - peak_score)
    totals = lax.optimization_barrier(jnp.sum(weights, axis=-1))
    rounded = lax.optimization_barrier(weights.astype(jnp.bfloat16)).astype(jnp.float32)
    numerators = jnp.einsum('hmqk,khv->hmqv', rounded, value_view)
    heads_out = numerators / totals[..., None]
    combined = heads_out[:, 0] - lambdas[:, None, None] * heads_out[:, 1]
    mean_square = lax.optimization_barrier(jnp.mean(combined * combined, axis=-1, keepdims=True))
    normalized = combined * lax.rsqrt(mean_square + EPSILON) * head_gain * OUT_SCALE
    return jnp.transpose(normalized, (1, 0, 2)).reshape(query_block.shape[0], -1).astype(jnp.bfloat16)

def attend_sequence(operands, lambdas, head_gain):
    seq_queries, seq_keys, seq_values = operands
    query_view = seq_queries.reshape(SEQ_LEN // 128, 128, HEADS, 2, HEAD_DIM)
    key_view = seq_keys.reshape(SEQ_LEN, HEADS, 2, HEAD_DIM).astype(jnp.float32)
    value_view = seq_values.reshape(SEQ_LEN, HEADS, 2 * HEAD_DIM).astype(jnp.float32)
    return lax.map(lambda query_block: attend_block(query_block, key_view, value_view, lambdas, head_gain), query_view)

def run_expert(operands):
    rows_in, gate_weight, up_weight, down_weight = operands
    gate_proj = jnp.dot(rows_in, gate_weight, preferred_element_type=jnp.float32)
    up_proj = jnp.dot(rows_in, up_weight, preferred_element_type=jnp.float32)
    hidden_units = (jax.nn.silu(gate_proj) * up_proj).astype(jnp.bfloat16)
    return jnp.dot(hidden_units, down_weight.T, preferred_element_type=jnp.float32).astype(jnp.bfloat16)

def reference(queries, keys, values, lambdas, head_gain, w_out, residual_in, norm_gain, route_ids, route_weight, w_gate, w_up, w_down):
    width = HEADS * 2 * HEAD_DIM
    seq_shape = (SEQUENCES, SEQ_LEN, width)
    attended = lax.map(lambda operands: attend_sequence(operands, lambdas, head_gain), (queries.reshape(seq_shape), keys.reshape(seq_shape), values.reshape(seq_shape)))
    attended = attended.reshape(TOKENS, width)
    mixed_out = jnp.dot(attended, w_out, preferred_element_type=jnp.float32).astype(jnp.bfloat16)
    carried = (residual_in.astype(jnp.float32) + mixed_out.astype(jnp.float32)).astype(jnp.bfloat16)
    carried_wide = carried.astype(jnp.float32)
    normed = (carried_wide * lax.rsqrt(lax.optimization_barrier(jnp.mean(carried_wide * carried_wide, axis=-1, keepdims=True)) + EPSILON) * norm_gain).astype(jnp.bfloat16)
    blocks = TOKENS // DEV_ROWS
    flat_ids = route_ids.reshape(blocks, 2 * DEV_ROWS)
    slot_index = jax.vmap(slot_numbers)(flat_ids)
    targets = (flat_ids * CAPACITY + slot_index).astype(jnp.int32)
    sources = jnp.repeat(normed.reshape(blocks, DEV_ROWS, D), 2, axis=1)
    block_index = jnp.broadcast_to(jnp.arange(blocks, dtype=jnp.int32)[:, None], targets.shape)
    buffers = jnp.zeros((blocks, EXPERTS * CAPACITY, D), jnp.bfloat16).at[block_index, targets].set(sources)
    per_expert = jnp.moveaxis(buffers.reshape(blocks, EXPERTS, CAPACITY, D), 1, 0).reshape(EXPERTS, blocks * CAPACITY, D)
    outputs = lax.map(run_expert, (per_expert, w_gate, w_up, w_down))
    returned = jnp.moveaxis(outputs.reshape(EXPERTS, blocks, CAPACITY, D), 0, 1).reshape(blocks, EXPERTS * CAPACITY, D)
    picked = returned[block_index, targets].astype(jnp.float32).reshape(TOKENS, 2, D)
    layer_out = carried.astype(jnp.float32) + lax.optimization_barrier(jnp.sum(route_weight[..., None] * picked, axis=1))
    return layer_out.astype(jnp.bfloat16)
```

```python
import functools
import jax
import jax.numpy as jnp
from jax import lax
from jax.experimental import pallas as pl
from jax.experimental.pallas import tpu as pltpu
from jax.sharding import PartitionSpec as P

EPSILON = 1e-06
OUT_SCALE = 0.8
FLOOR_SCORE = -1e30
LOG2E = 1.4426950408889634
MESH = pl.DeviceIdType.MESH


def attend_kernel(lam_ref, gain_ref, q_ref, k_ref, v_ref, o_ref,
                  kbuf, vbuf, qbuf, qz, sbuf, ebuf, acc, mrun, att,
                  ssem, rsem, qsem, osend, orecv):
    s = lax.axis_index("sp")
    x = lax.axis_index("tp")
    rows = q_ref.shape[2]
    zb = (s // 8) % 2
    y = (s // 2) % 4
    c = s % 2
    mine = s % 16
    base = s - mine
    y1 = y + 1 - 2 * (y % 2)
    y3 = 3 - y
    y2 = (y + 2) % 4

    def slot_of(zz, yy, cc):
        return zz * 8 + yy * 2 + cc

    zpeer = base + slot_of(1 - zb, y, c)
    y1dev = base + slot_of(zb, y1, c)
    y3dev = base + slot_of(zb, y3, c)
    twin = base + slot_of(zb, y, 1 - c)

    barrier = pltpu.get_barrier_semaphore()
    peers = [(zpeer, x), (y1dev, x), (y3dev, x), (twin, x)]
    for j in range(1, 4):
        peers.append((s, (x + j) % 4))
        peers.append((zpeer, (x + j) % 4))
    for ps, px in peers:
        pl.semaphore_signal(barrier, inc=1, device_id={"sp": ps, "tp": px}, device_id_type=MESH)
    pl.semaphore_wait(barrier, len(peers))

    def kslot(slot):
        return kbuf.at[slot // 2, pl.ds(pl.multiple_of((slot % 2) * rows, rows), rows)]

    def vslot(slot):
        return vbuf.at[slot, pl.ds(0, 128)]

    def pair_copy(ksrc, vsrc, slot, dest, idx):
        return (
            pltpu.make_async_remote_copy(ksrc, kslot(slot), ssem.at[idx, 0], rsem.at[slot, 0],
                                         device_id={"sp": dest, "tp": x}, device_id_type=MESH),
            pltpu.make_async_remote_copy(vsrc, vslot(slot), ssem.at[idx, 1], rsem.at[slot, 1],
                                         device_id={"sp": dest, "tp": x}, device_id_type=MESH),
        )

    def start(pair):
        pair[0].start()
        pair[1].start()

    def forward(slot, dest, idx):
        start(pair_copy(kslot(slot), vslot(slot), slot, dest, idx))

    def wait_slot(slot):
        a, b = pair_copy(kslot(slot), vslot(slot), slot, twin, 0)
        a.wait_recv()
        b.wait_recv()

    qcopy = pltpu.make_async_remote_copy(q_ref.at[1 - zb], qbuf, qsem.at[0], qsem.at[1],
                                         device_id={"sp": zpeer, "tp": x}, device_id_type=MESH)
    qcopy.start()
    own_k, own_v = k_ref.at[zb], v_ref.at[zb]
    start(pair_copy(own_k, own_v, mine, twin, 3))
    start(pair_copy(k_ref.at[1 - zb], v_ref.at[1 - zb], mine, zpeer, 0))
    start(pair_copy(own_k, own_v, mine, y1dev, 1))
    start(pair_copy(own_k, own_v, mine, y3dev, 2))

    kbuf[mine // 2, pl.ds(pl.multiple_of(c * rows, rows), rows), :] = k_ref[zb]
    vbuf[mine, pl.ds(0, 128), :] = v_ref[zb]
    for slot in range(16):
        vbuf[slot, pl.ds(128, 16), :] = jnp.ones((16, rows), jnp.bfloat16)
    zeros = jnp.zeros((64, rows), jnp.bfloat16)

    def put_queries(value, column):
        qz[pl.ds(0, 64), pl.ds(column, rows)] = value[:64]
        qz[pl.ds(64, 64), pl.ds(column, rows)] = zeros
        qz[pl.ds(0, 64), pl.ds(2 * rows + column, rows)] = zeros
        qz[pl.ds(64, 64), pl.ds(2 * rows + column, rows)] = value[64:]

    put_queries(q_ref[zb], 0)
    mrun[...] = jnp.full(mrun.shape, FLOOR_SCORE, jnp.float32)
    acc[...] = jnp.zeros(acc.shape, jnp.float32)
    qcopy.wait_recv()
    put_queries(qbuf[...], rows)

    scale = LOG2E * 64 ** (-0.5)
    keys_here = 2 * rows
    tiles = 2 * 2 * rows // 256
    per_map = tiles // 2

    def scores(p, t):
        column = t * 256
        top = None
        for part in range(2):
            value = jnp.dot(kbuf[p, pl.ds(part * rows, rows), :], qz[:, pl.ds(column, 256)],
                            preferred_element_type=jnp.float32)
            sbuf[t % 2, pl.ds(part * rows, rows), :] = value
            peak = jnp.max(value.reshape(rows // 8, 8, 256), axis=0)
            top = peak if top is None else jnp.maximum(top, peak)
        return jnp.max(top, axis=0, keepdims=True) * scale

    def weigh(t, peak):
        old = mrun[t]
        new = jnp.maximum(old, peak)
        mrun[t] = new
        for part in range(4):
            here = pl.ds(part * keys_here // 4, keys_here // 4)
            ebuf[t % 2, here, :] = jnp.exp2(sbuf[t % 2, here, :] * scale - new).astype(jnp.bfloat16)
        return jnp.exp2(old - new)

    def gather_values(p, t, shrink):
        product = jnp.dot(vbuf[2 * p], ebuf[t % 2, pl.ds(0, rows), :], preferred_element_type=jnp.float32)
        product += jnp.dot(vbuf[2 * p + 1], ebuf[t % 2, pl.ds(rows, rows), :], preferred_element_type=jnp.float32)
        acc[t] = acc[t] * shrink + product

    def compute(p):
        peak = scores(p, 0)
        for t in range(tiles):
            following = scores(p, t + 1) if t + 1 < tiles else None
            shrink = weigh(t, peak)
            gather_values(p, t, shrink)
            peak = following

    order = [(0, y), (1, y), (0, y1), (1, y1), (0, y3), (1, y3), (0, y2), (1, y2)]

    def comm(i):
        flip, yy = order[i]
        zz = zb + flip - 2 * zb * flip
        slot = slot_of(zz, yy, c)
        wait_slot(slot)
        if i == 1:
            forward(slot, y1dev, 4)
            forward(slot, y3dev, 5)
        if i == 2:
            forward(slot, y3dev, 8)
        if i == 5:
            forward(slot, y1dev, 12)
        forward(slot, twin, {1: 6, 2: 7, 3: 9, 4: 10, 5: 11, 6: 13, 7: 14}[i])

    def step(i, carry):
        @pl.when(i == 1)
        def _():
            comm(1)
            comm(2)
        for k in range(3, 8):
            @pl.when(i == k - 1)
            def _(k=k):
                comm(k)
        j = i // 2
        gray = j + (j // 2) - 2 * (j // 2) * (j % 2)
        lo, hi = gray % 2, gray // 2
        yhi, ylo = y // 2, y % 2
        yy = 2 * (yhi + hi - 2 * yhi * hi) + (ylo + lo - 2 * ylo * lo)
        flip = i % 2
        zz = zb + flip - 2 * zb * flip
        wait_slot(slot_of(zz, yy, 1 - c))
        compute(zz * 4 + yy)
        return carry

    lax.fori_loop(0, 8, step, 0)

    lam = lam_ref[0, 0]
    gain = gain_ref[...]
    head = 2 * x + zb
    for qt in (2, 3, 0, 1):
        first, second = acc[qt], acc[per_map + qt]
        combined = first[:128] / first[128:129] - lam * (second[:128] / second[128:129])
        mean_square = jnp.mean(combined * combined, axis=0, keepdims=True)
        value = (combined * lax.rsqrt(mean_square + EPSILON) * gain).astype(jnp.bfloat16)
        att[2 * qt] = value[:, :128]
        att[2 * qt + 1] = value[:, 128:]

    sends = []
    for j in range(4):
        xx = (x + j) % 4
        sends.append(pltpu.make_async_remote_copy(
            att.at[4 + xx], o_ref.at[head], osend.at[j], orecv.at[head],
            device_id={"sp": zpeer, "tp": xx}, device_id_type=MESH))
        sends[-1].start()
    for j in range(1, 4):
        xx = (x + j) % 4
        sends.append(pltpu.make_async_remote_copy(
            att.at[xx], o_ref.at[head], osend.at[3 + j], orecv.at[head],
            device_id={"sp": s, "tp": xx}, device_id_type=MESH))
        sends[-1].start()
    o_ref[head] = att[x]
    for j in range(4):
        xx = (x + j) % 4
        for far in range(2):
            if j == 0 and far == 0:
                continue
            hh = 2 * xx + (1 - zb if far else zb)
            pltpu.make_async_remote_copy(
                att.at[0], o_ref.at[hh], osend.at[0], orecv.at[hh],
                device_id={"sp": zpeer, "tp": x}, device_id_type=MESH).wait_recv()
    for copy in sends:
        copy.wait_send()
    qcopy.wait_send()
    for idx in range(15):
        a, b = pair_copy(own_k, own_v, mine, twin, idx)
        a.wait_send()
        b.wait_send()


def attend(queries, keys, values, lambdas, head_gain):
    rows = queries.shape[0]
    zb = (lax.axis_index("sp") // 8) % 2
    q = jnp.transpose(queries.reshape(rows, 2, 128), (1, 2, 0))
    k = jnp.transpose(keys.reshape(rows, 2, 128), (1, 0, 2))
    v = jnp.transpose(values.reshape(rows, 2, 128), (1, 2, 0))
    lam = lax.dynamic_slice(lambdas, (zb,), (1,)).reshape(1, 1)
    gain = (head_gain * OUT_SCALE).reshape(128, 1)
    bf, f32 = jnp.bfloat16, jnp.float32
    tiles = 4 * rows // 256
    vm = pl.BlockSpec(memory_space=pltpu.VMEM)
    return pl.pallas_call(
        attend_kernel,
        out_shape=jax.ShapeDtypeStruct((8, 128, 128), bf),
        in_specs=[pl.BlockSpec(memory_space=pltpu.SMEM), vm, vm, vm, vm],
        out_specs=vm,
        scratch_shapes=[
            pltpu.VMEM((8, 2 * rows, 128), bf),
            pltpu.VMEM((16, 144, rows), bf),
            pltpu.VMEM((128, rows), bf),
            pltpu.VMEM((128, 4 * rows), bf),
            pltpu.VMEM((2, 2 * rows, 256), f32),
            pltpu.VMEM((2, 2 * rows, 256), bf),
            pltpu.VMEM((tiles, 144, 256), f32),
            pltpu.VMEM((tiles, 1, 256), f32),
            pltpu.VMEM((8, 128, 128), bf),
            pltpu.SemaphoreType.DMA((15, 2)),
            pltpu.SemaphoreType.DMA((16, 2)),
            pltpu.SemaphoreType.DMA((2,)),
            pltpu.SemaphoreType.DMA((7,)),
            pltpu.SemaphoreType.DMA((8,)),
        ],
        compiler_params=pltpu.CompilerParams(collective_id=1, has_side_effects=True,
                                             vmem_limit_bytes=40 * 1024 * 1024),
        name="attend",
    )(lam, gain, q, k, v)


def slot_numbers(flat_ids):
    count_ids = flat_ids.shape[0]
    positions = lax.broadcasted_iota(jnp.int32, (count_ids, count_ids), 0)
    earlier = lax.broadcasted_iota(jnp.int32, (count_ids, count_ids), 1) < positions
    matches = (flat_ids[:, None] == flat_ids[None, :]) & earlier
    return jnp.sum(matches.astype(jnp.int32), axis=1)


def expert_hidden(arrived, gate_weight, up_weight):
    gate_proj = jnp.einsum("secd,edf->secf", arrived, gate_weight, preferred_element_type=jnp.float32)
    up_proj = jnp.einsum("secd,edf->secf", arrived, up_weight, preferred_element_type=jnp.float32)
    return (jax.nn.silu(gate_proj) * up_proj).astype(jnp.bfloat16)


def send_back(results):
    return lax.all_to_all(results, "sp", split_axis=0, concat_axis=0, tiled=True)


def local(queries, keys, values, lambdas, head_gain, w_out, residual_in, norm_gain,
          route_ids, route_weight, w_gate, w_up, w_down):
    attended = attend(queries, keys, values, lambdas, head_gain).reshape(8 * 128, 128)
    dev_rows = residual_in.shape[0]
    mixed_sum = lax.dot_general(attended, w_out, (((0,), (0,)), ((), ())), preferred_element_type=jnp.float32)
    mixed_out = mixed_sum.astype(jnp.bfloat16)
    carried = (residual_in.astype(jnp.float32) + mixed_out.astype(jnp.float32)).astype(jnp.bfloat16)
    carried_wide = carried.astype(jnp.float32)
    normed = (
        carried_wide
        * lax.rsqrt(jnp.mean(carried_wide * carried_wide, axis=-1, keepdims=True) + EPSILON)
        * norm_gain
    ).astype(jnp.bfloat16)
    model_width = normed.shape[1]
    experts_here = w_gate.shape[0]
    expert_count = experts_here * lax.axis_size("sp")
    capacity = max(2, 4 * dev_rows // expert_count)
    flat_ids = route_ids.reshape(-1)
    targets = flat_ids * capacity + slot_numbers(flat_ids)
    slot_ids = lax.broadcasted_iota(jnp.int32, (expert_count * capacity, dev_rows, 2), 0)
    placement_matrix = jnp.sum(
        (targets.reshape(1, dev_rows, 2) == slot_ids).astype(jnp.int32), axis=2
    ).astype(jnp.bfloat16)
    outgoing = jnp.dot(placement_matrix, normed, preferred_element_type=jnp.float32).astype(jnp.bfloat16)
    outgoing = outgoing.reshape(lax.axis_size("sp"), experts_here, capacity, model_width)
    full_gate, full_up, full_down = (
        lax.all_gather(w_gate, "tp", axis=2, tiled=True),
        lax.all_gather(w_up, "tp", axis=2, tiled=True),
        lax.all_gather(w_down, "tp", axis=2, tiled=True),
    )
    hidden_units = expert_hidden(
        lax.all_to_all(outgoing, "sp", split_axis=0, concat_axis=0, tiled=True), full_gate, full_up
    )
    summed = jnp.einsum("secf,edf->secd", hidden_units, full_down, preferred_element_type=jnp.float32)
    returned = send_back(summed.astype(jnp.bfloat16))
    flat_back = returned.reshape(expert_count * capacity, model_width)
    picked = jnp.take(flat_back, targets, axis=0).astype(jnp.float32).reshape(dev_rows, 2, model_width)
    layer_out = carried_wide + jnp.sum(route_weight[..., None] * picked, axis=1)
    return layer_out.astype(jnp.bfloat16)


def solution(mesh):
    placed = (
        P("sp", "tp"), P("sp", "tp"), P("sp", "tp"), P("tp"), P(), P(),
        P(("sp", "tp"), None), P(), P(("sp", "tp"), None), P(("sp", "tp"), None),
        P("sp", None, "tp"), P("sp", None, "tp"), P("sp", None, "tp"),
    )
    return jax.shard_map(local, mesh=mesh, in_specs=placed, out_specs=P(("sp", "tp"), None), check_vma=False)
```

```python
import functools
import jax
import jax.numpy as jnp
from jax import lax
from jax.experimental import pallas as pl
from jax.experimental.pallas import tpu as pltpu
from jax.sharding import PartitionSpec as P

EPSILON = 1e-06
OUT_SCALE = 0.8
FLOOR_SCORE = -1e30
LOG2E = 1.4426950408889634
MESH = pl.DeviceIdType.MESH


class WeightExchange:
    def __init__(self, s, x, sources, fulls, send, recv):
        self.s, self.x, self.sources, self.fulls, self.send, self.recv = s, x, sources, fulls, send, recv
        self.side = x // 2
        self.home = s % 2 == self.side
        self.away = s % 2 != self.side
        self.beside = x + 1 - 2 * (x % 2)
        self.opposite = 3 - x
        self.twin = s + 1 - 2 * (s % 2)

    def copy(self, m, source, quarter, sp, tp, idx):
        return pltpu.make_async_remote_copy(
            source, self.fulls[m].at[quarter], self.send.at[m, idx], self.recv.at[m, quarter],
            device_id={"sp": sp, "tp": tp}, device_id_type=MESH)

    def wait(self, m, quarter):
        self.copy(m, self.fulls[m].at[quarter], quarter, self.twin, self.x, 0).wait_recv()

    def begin(self):
        @pl.when(self.home)
        def _():
            for m, source in enumerate(self.sources):
                self.copy(m, source.at[0], self.x, self.s, self.beside, 0).start()
                self.copy(m, source.at[0], self.x, self.twin, self.x, 1).start()

        @pl.when(self.away)
        def _():
            for m, source in enumerate(self.sources):
                self.copy(m, source.at[0], self.x, self.s, self.opposite, 0).start()

    def cross(self, m):
        @pl.when(self.home)
        def _():
            self.wait(m, self.opposite)
            block = self.fulls[m].at[self.opposite]
            self.copy(m, block, self.opposite, self.s, self.beside, 2).start()
            self.copy(m, block, self.opposite, self.twin, self.x, 3).start()

    def near(self, m):
        @pl.when(self.home)
        def _():
            self.wait(m, self.beside)
            self.copy(m, self.fulls[m].at[self.beside], self.beside, self.twin, self.x, 4).start()

    def far(self, m):
        quarter = 3 - self.beside

        @pl.when(self.home)
        def _():
            self.wait(m, quarter)
            self.copy(m, self.fulls[m].at[quarter], quarter, self.twin, self.x, 5).start()

    def finish(self):
        for m in range(len(self.sources)):
            block = self.sources[m].at[0]

            @pl.when(self.home)
            def _(m=m, block=block):
                for idx in range(6):
                    self.copy(m, block, self.x, self.twin, self.x, idx).wait_send()

            @pl.when(self.away)
            def _(m=m, block=block):
                self.copy(m, block, self.x, self.twin, self.x, 0).wait_send()
                for quarter in range(4):
                    self.wait(m, quarter)


def attend_kernel(lam_ref, gain_ref, q_ref, k_ref, v_ref, wg_ref, wu_ref, o_ref, fg_ref, fu_ref,
                  kbuf, vbuf, qbuf, qz, sbuf, ebuf, acc, mrun, att,
                  ssem, rsem, qsem, osend, orecv, wsend, wrecv):
    s = lax.axis_index("sp")
    x = lax.axis_index("tp")
    rows = q_ref.shape[2]
    zb = (s // 8) % 2
    y = (s // 2) % 4
    c = s % 2
    mine = s % 16
    base = s - mine
    y1 = y + 1 - 2 * (y % 2)
    y3 = 3 - y
    y2 = (y + 2) % 4

    def slot_of(zz, yy, cc):
        return zz * 8 + yy * 2 + cc

    zpeer = base + slot_of(1 - zb, y, c)
    y1dev = base + slot_of(zb, y1, c)
    y3dev = base + slot_of(zb, y3, c)
    twin = base + slot_of(zb, y, 1 - c)

    barrier = pltpu.get_barrier_semaphore()
    peers = [(zpeer, x), (y1dev, x), (y3dev, x), (twin, x)]
    for j in range(1, 4):
        peers.append((s, (x + j) % 4))
        peers.append((zpeer, (x + j) % 4))
    for ps, px in peers:
        pl.semaphore_signal(barrier, inc=1, device_id={"sp": ps, "tp": px}, device_id_type=MESH)
    pl.semaphore_wait(barrier, len(peers))

    def kslot(slot):
        return kbuf.at[slot // 2, pl.ds(pl.multiple_of((slot % 2) * rows, rows), rows)]

    def vslot(slot):
        return vbuf.at[slot, pl.ds(0, 128)]

    def pair_copy(ksrc, vsrc, slot, dest, idx):
        return (
            pltpu.make_async_remote_copy(ksrc, kslot(slot), ssem.at[idx, 0], rsem.at[slot, 0],
                                         device_id={"sp": dest, "tp": x}, device_id_type=MESH),
            pltpu.make_async_remote_copy(vsrc, vslot(slot), ssem.at[idx, 1], rsem.at[slot, 1],
                                         device_id={"sp": dest, "tp": x}, device_id_type=MESH),
        )

    def start(pair):
        pair[0].start()
        pair[1].start()

    def forward(slot, dest, idx):
        start(pair_copy(kslot(slot), vslot(slot), slot, dest, idx))

    def wait_slot(slot):
        a, b = pair_copy(kslot(slot), vslot(slot), slot, twin, 0)
        a.wait_recv()
        b.wait_recv()

    qcopy = pltpu.make_async_remote_copy(q_ref.at[1 - zb], qbuf, qsem.at[0], qsem.at[1],
                                         device_id={"sp": zpeer, "tp": x}, device_id_type=MESH)
    qcopy.start()
    own_k, own_v = k_ref.at[zb], v_ref.at[zb]
    start(pair_copy(own_k, own_v, mine, twin, 3))
    start(pair_copy(k_ref.at[1 - zb], v_ref.at[1 - zb], mine, zpeer, 0))
    start(pair_copy(own_k, own_v, mine, y1dev, 1))
    start(pair_copy(own_k, own_v, mine, y3dev, 2))

    weights = WeightExchange(s, x, (wg_ref, wu_ref), (fg_ref, fu_ref), wsend, wrecv)
    weights.begin()

    kbuf[mine // 2, pl.ds(pl.multiple_of(c * rows, rows), rows), :] = k_ref[zb]
    vbuf[mine, pl.ds(0, 128), :] = v_ref[zb]
    for slot in range(16):
        vbuf[slot, pl.ds(128, 16), :] = jnp.ones((16, rows), jnp.bfloat16)
    zeros = jnp.zeros((64, rows), jnp.bfloat16)

    def put_queries(value, column):
        qz[pl.ds(0, 64), pl.ds(column, rows)] = value[:64]
        qz[pl.ds(64, 64), pl.ds(column, rows)] = zeros
        qz[pl.ds(0, 64), pl.ds(2 * rows + column, rows)] = zeros
        qz[pl.ds(64, 64), pl.ds(2 * rows + column, rows)] = value[64:]

    put_queries(q_ref[zb], 0)
    mrun[...] = jnp.full(mrun.shape, FLOOR_SCORE, jnp.float32)
    acc[...] = jnp.zeros(acc.shape, jnp.float32)
    qcopy.wait_recv()
    put_queries(qbuf[...], rows)

    scale = LOG2E * 64 ** (-0.5)
    keys_here = 2 * rows
    tiles = 2 * 2 * rows // 256
    per_map = tiles // 2

    def scores(p, t):
        column = t * 256
        top = None
        for part in range(2):
            value = jnp.dot(kbuf[p, pl.ds(part * rows, rows), :], qz[:, pl.ds(column, 256)],
                            preferred_element_type=jnp.float32)
            sbuf[t % 2, pl.ds(part * rows, rows), :] = value
            peak = jnp.max(value.reshape(rows // 8, 8, 256), axis=0)
            top = peak if top is None else jnp.maximum(top, peak)
        return jnp.max(top, axis=0, keepdims=True) * scale

    def weigh(t, peak):
        old = mrun[t]
        new = jnp.maximum(old, peak)
        mrun[t] = new
        for part in range(4):
            here = pl.ds(part * keys_here // 4, keys_here // 4)
            ebuf[t % 2, here, :] = jnp.exp2(sbuf[t % 2, here, :] * scale - new).astype(jnp.bfloat16)
        return jnp.exp2(old - new)

    def gather_values(p, t, shrink):
        product = jnp.dot(vbuf[2 * p], ebuf[t % 2, pl.ds(0, rows), :], preferred_element_type=jnp.float32)
        product += jnp.dot(vbuf[2 * p + 1], ebuf[t % 2, pl.ds(rows, rows), :], preferred_element_type=jnp.float32)
        acc[t] = acc[t] * shrink + product

    def compute(p):
        peak = scores(p, 0)
        for t in range(tiles):
            following = scores(p, t + 1) if t + 1 < tiles else None
            shrink = weigh(t, peak)
            gather_values(p, t, shrink)
            peak = following

    order = [(0, y), (1, y), (0, y1), (1, y1), (0, y3), (1, y3), (0, y2), (1, y2)]

    def comm(i):
        flip, yy = order[i]
        zz = zb + flip - 2 * zb * flip
        slot = slot_of(zz, yy, c)
        wait_slot(slot)
        if i == 1:
            forward(slot, y1dev, 4)
            forward(slot, y3dev, 5)
        if i == 2:
            forward(slot, y3dev, 8)
        if i == 5:
            forward(slot, y1dev, 12)
        forward(slot, twin, {1: 6, 2: 7, 3: 9, 4: 10, 5: 11, 6: 13, 7: 14}[i])

    def step(i, carry):
        @pl.when(i == 1)
        def _():
            comm(1)
            comm(2)
        for k in range(3, 8):
            @pl.when(i == k - 1)
            def _(k=k):
                comm(k)
        @pl.when(i == 3)
        def _():
            weights.cross(0)
            weights.near(0)

        @pl.when(i == 5)
        def _():
            weights.cross(1)
            weights.near(1)

        @pl.when(i == 7)
        def _():
            weights.far(0)
        j = i // 2
        gray = j + (j // 2) - 2 * (j // 2) * (j % 2)
        lo, hi = gray % 2, gray // 2
        yhi, ylo = y // 2, y % 2
        yy = 2 * (yhi + hi - 2 * yhi * hi) + (ylo + lo - 2 * ylo * lo)
        flip = i % 2
        zz = zb + flip - 2 * zb * flip
        wait_slot(slot_of(zz, yy, 1 - c))
        compute(zz * 4 + yy)
        return carry

    lax.fori_loop(0, 8, step, 0)

    lam = lam_ref[0, 0]
    gain = gain_ref[...]
    head = 2 * x + zb
    for qt in (2, 3, 0, 1):
        first, second = acc[qt], acc[per_map + qt]
        combined = first[:128] / first[128:129] - lam * (second[:128] / second[128:129])
        mean_square = jnp.mean(combined * combined, axis=0, keepdims=True)
        value = (combined * lax.rsqrt(mean_square + EPSILON) * gain).astype(jnp.bfloat16)
        att[2 * qt] = value[:, :128]
        att[2 * qt + 1] = value[:, 128:]

    sends = []
    for j in range(4):
        xx = (x + j) % 4
        sends.append(pltpu.make_async_remote_copy(
            att.at[4 + xx], o_ref.at[head], osend.at[j], orecv.at[head],
            device_id={"sp": zpeer, "tp": xx}, device_id_type=MESH))
        sends[-1].start()
    for j in range(1, 4):
        xx = (x + j) % 4
        sends.append(pltpu.make_async_remote_copy(
            att.at[xx], o_ref.at[head], osend.at[3 + j], orecv.at[head],
            device_id={"sp": s, "tp": xx}, device_id_type=MESH))
        sends[-1].start()
    o_ref[head] = att[x]
    for j in range(4):
        xx = (x + j) % 4
        for far in range(2):
            if j == 0 and far == 0:
                continue
            hh = 2 * xx + (1 - zb if far else zb)
            pltpu.make_async_remote_copy(
                att.at[0], o_ref.at[hh], osend.at[0], orecv.at[hh],
                device_id={"sp": zpeer, "tp": x}, device_id_type=MESH).wait_recv()
    weights.far(1)
    for copy in sends:
        copy.wait_send()
    qcopy.wait_send()
    weights.finish()
    for idx in range(15):
        a, b = pair_copy(own_k, own_v, mine, twin, idx)
        a.wait_send()
        b.wait_send()


def attend(queries, keys, values, lambdas, head_gain, w_gate, w_up):
    rows = queries.shape[0]
    zb = (lax.axis_index("sp") // 8) % 2
    q = jnp.transpose(queries.reshape(rows, 2, 128), (1, 2, 0))
    k = jnp.transpose(keys.reshape(rows, 2, 128), (1, 0, 2))
    v = jnp.transpose(values.reshape(rows, 2, 128), (1, 2, 0))
    lam = lax.dynamic_slice(lambdas, (zb,), (1,)).reshape(1, 1)
    gain = (head_gain * OUT_SCALE).reshape(128, 1)
    bf, f32 = jnp.bfloat16, jnp.float32
    tiles = 4 * rows // 256
    vm = pl.BlockSpec(memory_space=pltpu.VMEM)
    hbm = pl.BlockSpec(memory_space=pltpu.HBM)
    return pl.pallas_call(
        attend_kernel,
        out_shape=(jax.ShapeDtypeStruct((8, 128, 128), bf), jax.ShapeDtypeStruct((4,) + w_gate.shape[1:], bf),
                   jax.ShapeDtypeStruct((4,) + w_up.shape[1:], bf)),
        in_specs=[pl.BlockSpec(memory_space=pltpu.SMEM), vm, vm, vm, vm, hbm, hbm],
        out_specs=(vm, hbm, hbm),
        scratch_shapes=[
            pltpu.VMEM((8, 2 * rows, 128), bf),
            pltpu.VMEM((16, 144, rows), bf),
            pltpu.VMEM((128, rows), bf),
            pltpu.VMEM((128, 4 * rows), bf),
            pltpu.VMEM((2, 2 * rows, 256), f32),
            pltpu.VMEM((2, 2 * rows, 256), bf),
            pltpu.VMEM((tiles, 144, 256), f32),
            pltpu.VMEM((tiles, 1, 256), f32),
            pltpu.VMEM((8, 128, 128), bf),
            pltpu.SemaphoreType.DMA((15, 2)),
            pltpu.SemaphoreType.DMA((16, 2)),
            pltpu.SemaphoreType.DMA((2,)),
            pltpu.SemaphoreType.DMA((7,)),
            pltpu.SemaphoreType.DMA((8,)),
            pltpu.SemaphoreType.DMA((2, 6)),
            pltpu.SemaphoreType.DMA((2, 4)),
        ],
        compiler_params=pltpu.CompilerParams(collective_id=1, has_side_effects=True,
                                             vmem_limit_bytes=40 * 1024 * 1024),
        name="attend",
    )(lam, gain, q, k, v, w_gate, w_up)


Z_STEPS = (0, 1, 7, 2, 6, 3, 5, 4)


def expert_kernel(tok_in, meta_in, carried_ref, place_ref, fg_ref, fu_ref, wg_ref, wu_ref, wd_ref, o_ref,
                  tok, meta, ex, er, gw, uw, wd, hb, yb, rb, cb, fin,
                  tsend, trecv, msend, mrecv, esend, erecv, ysend, yrecv, fsend, frecv, wsem, dsend, drecv):
    s = lax.axis_index("sp")
    x = lax.axis_index("tp")
    z = s // 8
    y = (s // 2) % 4
    c = s % 2
    side = x // 2
    weights = WeightExchange(s, x, (wd_ref,), (wd,), dsend, drecv)

    def z_device(step):
        return ((z + step) % 8) * 8 + y * 2 + c

    def expert_of(k):
        which = k % 2
        stays = 1 - (which + side - 2 * which * side)
        return z * 8 + ((y + k // 2) % 4) * 2 + (1 - stays), stays * x + (1 - stays) * (3 - x)

    def expert_number(k):
        return ((y + k // 2) % 4) * 2 + k % 2

    plane = (1 - c) * x + c * (3 - x)

    def hub_of(h):
        return z * 8 + hub_number(h), plane

    def hub_number(h):
        return ((y + h // 2) % 4) * 2 + (c + h) % 2

    my_expert = y * 2 + side
    other = c == 1

    def self_expert(k):
        return k // 2 == 0

    def when_remote_expert(k, body):
        if k // 2 == 0:
            pl.when(jnp.logical_or(other, side != k % 2))(body)
        else:
            body()

    def when_remote_hub(h, body):
        if h == 0:
            pl.when(other)(body)
        else:
            body()

    barrier = pltpu.get_barrier_semaphore()

    def greet(sp, tp):
        pl.semaphore_signal(barrier, inc=1, device_id={"sp": sp, "tp": tp}, device_id_type=MESH)

    for step in range(1, 8):
        greet(z_device(step), x)
    for k in range(8):
        when_remote_expert(k, lambda k=k: greet(*expert_of(k)))
        when_remote_hub(k, lambda k=k: greet(*hub_of(k)))
    greet(s, weights.beside)
    greet(s, weights.opposite)
    greet(weights.twin, x)
    pl.semaphore_wait(barrier, 24 + 2 * c)

    def token_copies(n):
        dest = {"sp": z_device(Z_STEPS[n]), "tp": x}
        return (pltpu.make_async_remote_copy(tok_in.at[n], tok.at[n], tsend.at[n], trecv.at[n],
                                             device_id=dest, device_id_type=MESH),
                pltpu.make_async_remote_copy(meta_in.at[n], meta.at[n], msend.at[n], mrecv.at[n],
                                             device_id=dest, device_id_type=MESH))

    for n in range(1, 8):
        for copy in token_copies(n):
            copy.start()
    weights.begin()

    def load(m, source, target, q, sem):
        return pltpu.make_async_copy(source, target.at[q], wsem.at[m, sem])

    full_refs, own_refs, targets = (fg_ref, fu_ref), (wg_ref, wu_ref), (gw, uw)
    for m in range(2):
        for j in range(4):
            q = (x + j) % 4
            if j == 0:
                @pl.when(weights.home)
                def _(m=m, q=q):
                    load(m, own_refs[m].at[0], targets[m], q, 0).start()

                @pl.when(weights.away)
                def _(m=m, q=q):
                    load(m, full_refs[m].at[q], targets[m], q, 0).start()
            else:
                load(m, full_refs[m].at[q], targets[m], q, j).start()

    @pl.when(weights.home)
    def _():
        load(2, wd_ref.at[0], wd, x, 0).start()

    tok[0] = tok_in[0]
    meta[0] = meta_in[0]

    slot_rows = lax.broadcasted_iota(jnp.int32, (128, 32), 0).astype(jnp.float32)

    def chosen(n):
        first = slot_rows == meta[n, 0:1, 0:32] + 8.0 * (n % 2)
        second = slot_rows == meta[n, 1:2, 0:32] + 8.0 * (n % 2)
        return first, second

    def spread(n):
        first, second = chosen(n)
        return jnp.where(jnp.logical_or(first, second), 1.0, 0.0).astype(jnp.bfloat16)

    def expert_copy(p, k):
        sp, tp = expert_of(k)
        number = expert_number(k)
        return pltpu.make_async_remote_copy(
            ex.at[p, number], er.at[p, y * 2 + c], esend.at[p, k], erecv.at[p, y * 2 + c],
            device_id={"sp": sp, "tp": tp}, device_id_type=MESH)

    def dispatch(p):
        for n in (2 * p, 2 * p + 1):
            if n > 0:
                for copy in token_copies(n):
                    copy.wait_recv()
        even, odd = spread(2 * p), spread(2 * p + 1)
        for part in range(4):
            here = pl.ds(part * 512, 512)
            block = jnp.dot(even, tok[2 * p, :, here], preferred_element_type=jnp.float32)
            block += jnp.dot(odd, tok[2 * p + 1, :, here], preferred_element_type=jnp.float32)
            ex[p, :, :, here] = block.astype(jnp.bfloat16).reshape(8, 16, 512)
        for k in (0, 1, 2, 3, 6, 7, 4, 5):
            when_remote_expert(k, lambda k=k: expert_copy(p, k).start())

        @pl.when(jnp.logical_not(other))
        def _():
            er[p, y * 2] = ex[p, my_expert]

    dispatch(0)
    dispatch(1)
    weights.cross(0)
    weights.near(0)
    dispatch(2)
    dispatch(3)
    weights.far(0)

    for m in range(2):
        for j in range(4):
            load(m, own_refs[m].at[0], targets[m], x, j).wait()

    def expert_rows_wait(p):
        for h in range(8):
            number = hub_number(h)
            when_remote_hub(h, lambda number=number: pltpu.make_async_remote_copy(
                ex.at[p, 0], er.at[p, number], esend.at[p, 0], erecv.at[p, number],
                device_id={"sp": s, "tp": weights.beside}, device_id_type=MESH).wait_recv())

    def output_copy(p, h):
        sp, tp = hub_of(h)
        return pltpu.make_async_remote_copy(
            yb.at[p, hub_number(h)], rb.at[p, my_expert], ysend.at[p, h], yrecv.at[p, my_expert],
            device_id={"sp": sp, "tp": tp}, device_id_type=MESH)

    def hidden(half):
        def one_quarter(q, carry):
            rows = er[pl.ds(2 * half, 2)].reshape(256, 2048)
            gate = jnp.dot(rows, gw[q], preferred_element_type=jnp.float32)
            up = jnp.dot(rows, uw[q], preferred_element_type=jnp.float32)
            hb[q] = (gate / (1.0 + jnp.exp(-gate)) * up).astype(jnp.bfloat16)
            return carry
        lax.fori_loop(0, 4, one_quarter, 0)

    def outputs(half):
        for part in range(8):
            here = pl.ds(part * 256, 256)
            total = None
            for q in range(4):
                term = lax.dot_general(hb[q], wd[q, here, :], (((1,), (1,)), ((), ())),
                                       preferred_element_type=jnp.float32)
                total = term if total is None else total + term
            yb[pl.ds(2 * half, 2), :, :, here] = total.astype(jnp.bfloat16).reshape(2, 8, 16, 256)

    def send_back(p):
        for h in (0, 1, 2, 3, 6, 7, 4, 5):
            when_remote_hub(h, lambda h=h: output_copy(p, h).start())

        @pl.when(jnp.logical_not(other))
        def _():
            rb[p, my_expert] = yb[p, y * 2]

    def final_copy(n):
        dest = {"sp": z_device(8 - Z_STEPS[n]), "tp": x}
        return pltpu.make_async_remote_copy(cb.at[n], fin.at[n], fsend.at[n], frecv.at[n],
                                            device_id=dest, device_id_type=MESH)

    def combine(p):
        for k in range(8):
            number = expert_number(k)
            when_remote_expert(k, lambda number=number: pltpu.make_async_remote_copy(
                yb.at[p, 0], rb.at[p, number], ysend.at[p, 0], yrecv.at[p, number],
                device_id={"sp": s, "tp": weights.beside}, device_id_type=MESH).wait_recv())
        for n in (2 * p, 2 * p + 1):
            first, second = chosen(n)
            mix = jnp.where(first, meta[n, 2:3, 0:32], 0.0) + jnp.where(second, meta[n, 3:4, 0:32], 0.0)
            high = mix.astype(jnp.bfloat16)
            low = (mix - high.astype(jnp.float32)).astype(jnp.bfloat16)
            both = jnp.transpose(jnp.concatenate([high, low], axis=0).astype(jnp.float32)).astype(jnp.bfloat16)
            for part in range(4):
                here = pl.ds(part * 512, 512)
                rows = rb[p, :, :, here].reshape(128, 512)
                value = jnp.dot(both[:, :128], rows, preferred_element_type=jnp.float32)
                value += jnp.dot(both[:, 128:], rows, preferred_element_type=jnp.float32)
                cb[n, :, here] = value.astype(jnp.bfloat16)
            if n > 0:
                final_copy(n).start()

    for half in range(2):
        expert_rows_wait(2 * half)
        expert_rows_wait(2 * half + 1)
        hidden(half)
        if half == 0:
            @pl.when(weights.home)
            def _():
                load(2, wd_ref.at[0], wd, x, 0).wait()
            weights.finish()
        outputs(half)
        send_back(2 * half)
        send_back(2 * half + 1)
    for p in range(4):
        combine(p)

    for n in range(1, 8):
        final_copy(n).wait_recv()
    fin[0] = cb[0]
    places = lax.broadcasted_iota(jnp.int32, (128, 256), 1)
    pick = jnp.where(places == place_ref[...], 1.0, 0.0).astype(jnp.bfloat16)
    for part in range(4):
        here = pl.ds(part * 512, 512)
        value = jnp.dot(pick, fin[:, :, here].reshape(256, 512), preferred_element_type=jnp.float32)
        o_ref[:, here] = (carried_ref[:, here].astype(jnp.float32) + value).astype(jnp.bfloat16)

    for n in range(1, 8):
        for copy in token_copies(n):
            copy.wait_send()
        final_copy(n).wait_send()
    for p in range(4):
        for k in range(8):
            when_remote_expert(k, lambda k=k: expert_copy(p, k).wait_send())
            when_remote_hub(k, lambda k=k: output_copy(p, k).wait_send())


def experts(grouped, meta, carried, place, full_gate, full_up, w_gate, w_up, w_down):
    bf, f32 = jnp.bfloat16, jnp.float32
    vm = pl.BlockSpec(memory_space=pltpu.VMEM)
    hbm = pl.BlockSpec(memory_space=pltpu.HBM)
    dma = pltpu.SemaphoreType.DMA
    return pl.pallas_call(
        expert_kernel,
        out_shape=jax.ShapeDtypeStruct((128, 2048), bf),
        in_specs=[vm, vm, vm, vm, hbm, hbm, hbm, hbm, hbm],
        out_specs=vm,
        scratch_shapes=[
            pltpu.VMEM((8, 32, 2048), bf),
            pltpu.VMEM((8, 8, 128), f32),
            pltpu.VMEM((4, 8, 16, 2048), bf),
            pltpu.VMEM((4, 8, 16, 2048), bf),
            pltpu.VMEM((4, 2048, 256), bf),
            pltpu.VMEM((4, 2048, 256), bf),
            pltpu.VMEM((4, 2048, 256), bf),
            pltpu.VMEM((4, 256, 256), bf),
            pltpu.VMEM((4, 8, 16, 2048), bf),
            pltpu.VMEM((4, 8, 16, 2048), bf),
            pltpu.VMEM((8, 32, 2048), bf),
            pltpu.VMEM((8, 32, 2048), bf),
            dma((8,)), dma((8,)), dma((8,)), dma((8,)),
            dma((4, 8)), dma((4, 8)), dma((4, 8)), dma((4, 8)),
            dma((8,)), dma((8,)), dma((3, 4)), dma((1, 6)), dma((1, 4)),
        ],
        compiler_params=pltpu.CompilerParams(collective_id=2, has_side_effects=True,
                                             vmem_limit_bytes=56 * 1024 * 1024),
        name="experts",
    )(grouped, meta, carried, place, full_gate, full_up, w_gate, w_up, w_down)


def routing(route_ids, route_weight):
    rows = route_ids.shape[0]
    z = lax.axis_index("sp") // 8
    ids = jnp.transpose(route_ids)
    group = ids[0] // 8
    earlier = lax.broadcasted_iota(jnp.int32, (rows, rows), 0) < lax.broadcasted_iota(jnp.int32, (rows, rows), 1)

    def count(mask):
        return jnp.sum((mask & earlier).astype(jnp.int32), axis=0)

    same_first = (route_ids[:, 0:1] == ids[0:1]) | (route_ids[:, 1:2] == ids[0:1])
    same_second = (route_ids[:, 0:1] == ids[1:2]) | (route_ids[:, 1:2] == ids[1:2])
    same_group = (route_ids[:, 0:1] // 8) == group[None]
    slot0, slot1, position = count(same_first), count(same_second), count(same_group)
    away = (group - z + 8) % 8
    turn = jnp.where(away == 0, 0, jnp.where(away < 4, 2 * away - 1, 2 * (8 - away)))
    turn = jnp.where(away == 4, 7, turn)
    place = turn * 32 + position
    select = place[None, :] == lax.broadcasted_iota(jnp.int32, (8 * 32, rows), 0)
    facts = jnp.stack([
        ((ids[0] % 8) * 16 + slot0 + 1000).astype(jnp.float32),
        ((ids[1] % 8) * 16 + slot1 + 1000).astype(jnp.float32),
        route_weight[:, 0], route_weight[:, 1],
    ])
    table = jnp.sum(jnp.where(select[None], facts[:, None, :], 0.0), axis=2)
    table = jnp.concatenate([table[:2] - 1000.0, table[2:]], axis=0)
    meta = jnp.transpose(table.reshape(4, 8, 32), (1, 0, 2))
    return place.reshape(rows, 1), select.astype(jnp.bfloat16), jnp.pad(meta, ((0, 0), (0, 4), (0, 96)))


def local(queries, keys, values, lambdas, head_gain, w_out, residual_in, norm_gain,
          route_ids, route_weight, w_gate, w_up, w_down):
    attended, full_gate, full_up = attend(queries, keys, values, lambdas, head_gain, w_gate, w_up)
    place, select, meta = routing(route_ids, route_weight)
    mixed_sum = lax.dot_general(attended.reshape(8 * 128, 128), w_out, (((0,), (0,)), ((), ())),
                                preferred_element_type=jnp.float32)
    mixed_out = mixed_sum.astype(jnp.bfloat16)
    carried = (residual_in.astype(jnp.float32) + mixed_out.astype(jnp.float32)).astype(jnp.bfloat16)
    carried_wide = carried.astype(jnp.float32)
    normed = (
        carried_wide
        * lax.rsqrt(jnp.mean(carried_wide * carried_wide, axis=-1, keepdims=True) + EPSILON)
        * norm_gain
    ).astype(jnp.bfloat16)
    grouped = jnp.dot(select, normed, preferred_element_type=jnp.float32).astype(jnp.bfloat16)
    return experts(grouped.reshape(8, 32, -1), meta, carried, place, full_gate, full_up, w_gate, w_up, w_down)


def solution(mesh):
    placed = (
        P("sp", "tp"), P("sp", "tp"), P("sp", "tp"), P("tp"), P(), P(),
        P(("sp", "tp"), None), P(), P(("sp", "tp"), None), P(("sp", "tp"), None),
        P("sp", None, "tp"), P("sp", None, "tp"), P("sp", None, "tp"),
    )
    return jax.shard_map(local, mesh=mesh, in_specs=placed, out_specs=P(("sp", "tp"), None), check_vma=False)
```

```python
import functools
import jax
import jax.numpy as jnp
from jax import lax
from jax.experimental import pallas as pl
from jax.experimental.pallas import tpu as pltpu
from jax.sharding import PartitionSpec as P

EPSILON = 1e-06
OUT_SCALE = 0.8
FLOOR_SCORE = -1e30
LOG2E = 1.4426950408889634
MESH = pl.DeviceIdType.MESH


class WeightExchange:
    def __init__(self, s, x, places, send, recv):
        self.s, self.x, self.places, self.send, self.recv = s, x, places, send, recv
        self.side = x // 2
        self.home = s % 2 == self.side
        self.away = s % 2 != self.side
        self.beside = x + 1 - 2 * (x % 2)
        self.opposite = 3 - x
        self.twin = s + 1 - 2 * (s % 2)

    def copy(self, m, source, quarter, sp, tp, idx):
        return pltpu.make_async_remote_copy(
            source, self.places[m][quarter], self.send.at[m, idx], self.recv.at[m, quarter],
            device_id={"sp": sp, "tp": tp}, device_id_type=MESH)

    def wait(self, m, quarter):
        self.copy(m, self.places[m][quarter], quarter, self.twin, self.x, 0).wait_recv()

    def share(self, m, quarter, source=None):
        source = self.places[m][quarter] if source is None else source
        self.copy(m, source, quarter, self.twin, self.x, 2 + quarter).start()

    def begin(self, m, source):
        @pl.when(self.home)
        def _():
            self.copy(m, source, 1, self.s, self.beside, 0).start()
            self.share(m, 0, source)

        @pl.when(self.away)
        def _():
            self.copy(m, source, 2, self.s, self.opposite, 0).start()

    def pass_on(self, m, block=None):
        @pl.when(self.home)
        def _():
            self.copy(m, self.places[m][2] if block is None else block, 3, self.s, self.beside, 1).start()

    def landed(self, m, quarter):
        @pl.when(self.home)
        def _():
            self.wait(m, quarter)
            self.share(m, quarter)

    def finish(self, m, source, quarters):
        @pl.when(self.home)
        def _():
            if 1 in quarters:
                self.copy(m, source, 1, self.s, self.beside, 0).wait_send()
            if 3 in quarters:
                self.copy(m, source, 3, self.s, self.beside, 1).wait_send()
            for quarter in quarters:
                self.copy(m, source, quarter, self.twin, self.x, 2 + quarter).wait_send()

        @pl.when(self.away)
        def _():
            if 2 in quarters:
                self.copy(m, source, 2, self.s, self.opposite, 0).wait_send()
            for quarter in quarters:
                self.wait(m, quarter)


def attend_kernel(lam_ref, gain_ref, q_in, k_in, v_in, wout_hbm, res_ref, ngain_ref, ids_ref, rw_ref, wg_ref, wu_ref,
                  group_ref, facts_out, carried_ref, place_ref, fg_ref, fu_ref,
                  q_ref, v_ref, kbuf, vbuf, qbuf, qz, sbuf, ebuf, acc, mrun, att, o_ref, wout, facts,
                  ssem, rsem, qsem, osend, orecv, wsend, wrecv, lsem):
    s = lax.axis_index("sp")
    x = lax.axis_index("tp")
    rows = q_in.shape[0]
    zb = (s // 8) % 2
    y = (s // 2) % 4
    c = s % 2
    mine = s % 16
    base = s - mine
    y1 = y + 1 - 2 * (y % 2)
    y3 = 3 - y
    y2 = (y + 2) % 4

    def slot_of(zz, yy, cc):
        return zz * 8 + yy * 2 + cc

    zpeer = base + slot_of(1 - zb, y, c)
    y1dev = base + slot_of(zb, y1, c)
    y3dev = base + slot_of(zb, y3, c)
    twin = base + slot_of(zb, y, 1 - c)

    barrier = pltpu.get_barrier_semaphore()
    peers = [(zpeer, x), (y1dev, x), (y3dev, x), (twin, x)]
    for j in range(1, 4):
        peers.append((s, (x + j) % 4))
        peers.append((zpeer, (x + j) % 4))
    for ps, px in peers:
        pl.semaphore_signal(barrier, inc=1, device_id={"sp": ps, "tp": px}, device_id_type=MESH)
    for b in range(2):
        q_ref[b] = jnp.transpose(q_in[:, 128 * b:128 * (b + 1)])
        v_ref[b] = jnp.transpose(v_in[:, 128 * b:128 * (b + 1)])
    out_load = pltpu.make_async_copy(wout_hbm, wout, lsem.at[0])
    out_load.start()
    own_loads = (pltpu.make_async_copy(wg_ref.at[0], fg_ref.at[0], lsem.at[1]),
                 pltpu.make_async_copy(wu_ref.at[0], fu_ref.at[0], lsem.at[2]))
    pl.semaphore_wait(barrier, len(peers))

    def kslot(slot):
        return kbuf.at[slot // 2, pl.ds(pl.multiple_of((slot % 2) * rows, rows), rows)]

    def vslot(slot):
        return vbuf.at[slot, pl.ds(0, 128)]

    def pair_copy(ksrc, vsrc, slot, dest, idx):
        return (
            pltpu.make_async_remote_copy(ksrc, kslot(slot), ssem.at[idx, 0], rsem.at[slot, 0],
                                         device_id={"sp": dest, "tp": x}, device_id_type=MESH),
            pltpu.make_async_remote_copy(vsrc, vslot(slot), ssem.at[idx, 1], rsem.at[slot, 1],
                                         device_id={"sp": dest, "tp": x}, device_id_type=MESH),
        )

    def start(pair):
        pair[0].start()
        pair[1].start()

    def forward(slot, dest, idx):
        start(pair_copy(kslot(slot), vslot(slot), slot, dest, idx))

    def wait_slot(slot):
        a, b = pair_copy(kslot(slot), vslot(slot), slot, twin, 0)
        a.wait_recv()
        b.wait_recv()

    qcopy = pltpu.make_async_remote_copy(q_ref.at[1 - zb], qbuf, qsem.at[0], qsem.at[1],
                                         device_id={"sp": zpeer, "tp": x}, device_id_type=MESH)
    qcopy.start()

    def key_columns(b):
        return k_in.at[:, pl.ds(pl.multiple_of(b * 128, 128), 128)]

    own_k, own_v = key_columns(zb), v_ref.at[zb]
    start(pair_copy(own_k, own_v, mine, twin, 3))
    start(pair_copy(key_columns(1 - zb), v_ref.at[1 - zb], mine, zpeer, 0))
    start(pair_copy(own_k, own_v, mine, y1dev, 1))
    start(pair_copy(own_k, own_v, mine, y3dev, 2))

    weights = WeightExchange(s, x, ([fg_ref.at[i] for i in range(4)], [fu_ref.at[i] for i in range(3)]), wsend, wrecv)
    weights.begin(0, wg_ref.at[0])
    weights.begin(1, wu_ref.at[0])
    for own in own_loads:
        pl.when(weights.home)(own.start)

    kbuf[mine // 2, pl.ds(pl.multiple_of(c * rows, rows), rows), :] = key_columns(zb)[...]
    vbuf[mine, pl.ds(0, 128), :] = v_ref[zb]
    for slot in range(16):
        vbuf[slot, pl.ds(128, 16), :] = jnp.ones((16, rows), jnp.bfloat16)
    zeros = jnp.zeros((64, rows), jnp.bfloat16)

    def put_queries(value, column):
        qz[pl.ds(0, 64), pl.ds(column, rows)] = value[:64]
        qz[pl.ds(64, 64), pl.ds(column, rows)] = zeros
        qz[pl.ds(0, 64), pl.ds(2 * rows + column, rows)] = zeros
        qz[pl.ds(64, 64), pl.ds(2 * rows + column, rows)] = value[64:]

    put_queries(q_ref[zb], 0)
    mrun[...] = jnp.full(mrun.shape, FLOOR_SCORE, jnp.float32)
    acc[...] = jnp.zeros(acc.shape, jnp.float32)
    routing(z_of(s), ids_ref, rw_ref, facts, place_ref)
    qcopy.wait_recv()
    put_queries(qbuf[...], rows)

    scale = LOG2E * 64 ** (-0.5)
    keys_here = 2 * rows
    tiles = 2 * 2 * rows // 256
    per_map = tiles // 2

    def scores(p, t):
        column = t * 256
        top = None
        for part in range(2):
            value = jnp.dot(kbuf[p, pl.ds(part * rows, rows), :], qz[:, pl.ds(column, 256)],
                            preferred_element_type=jnp.float32)
            sbuf[t % 2, pl.ds(part * rows, rows), :] = value
            peak = jnp.max(value.reshape(rows // 8, 8, 256), axis=0)
            top = peak if top is None else jnp.maximum(top, peak)
        return jnp.max(top, axis=0, keepdims=True) * scale

    def weigh(t, peak):
        old = mrun[t]
        new = jnp.maximum(old, peak)
        mrun[t] = new
        for part in range(4):
            here = pl.ds(part * keys_here // 4, keys_here // 4)
            ebuf[t % 2, here, :] = jnp.exp2(sbuf[t % 2, here, :] * scale - new).astype(jnp.bfloat16)
        return jnp.exp2(old - new)

    def gather_values(p, t, shrink):
        product = jnp.dot(vbuf[2 * p], ebuf[t % 2, pl.ds(0, rows), :], preferred_element_type=jnp.float32)
        product += jnp.dot(vbuf[2 * p + 1], ebuf[t % 2, pl.ds(rows, rows), :], preferred_element_type=jnp.float32)
        acc[t] = acc[t] * shrink + product

    def compute(p):
        peak = scores(p, 0)
        for t in range(tiles):
            following = scores(p, t + 1) if t + 1 < tiles else None
            shrink = weigh(t, peak)
            gather_values(p, t, shrink)
            peak = following

    order = [(0, y), (1, y), (0, y1), (1, y1), (0, y3), (1, y3), (0, y2), (1, y2)]

    def comm(i):
        flip, yy = order[i]
        zz = zb + flip - 2 * zb * flip
        slot = slot_of(zz, yy, c)
        wait_slot(slot)
        if i == 1:
            forward(slot, y1dev, 4)
            forward(slot, y3dev, 5)
        if i == 2:
            forward(slot, y3dev, 8)
        if i == 5:
            forward(slot, y1dev, 12)
        forward(slot, twin, {1: 6, 2: 7, 3: 9, 4: 10, 5: 11, 6: 13, 7: 14}[i])

    def step(i, carry):
        @pl.when(i == 1)
        def _():
            comm(1)
            comm(2)
        for k in range(3, 8):
            @pl.when(i == k - 1)
            def _(k=k):
                comm(k)
        @pl.when(i == 3)
        def _():
            pl.when(weights.home)(lambda: weights.wait(0, 2))
            weights.pass_on(0)
            pl.when(weights.home)(lambda: weights.share(0, 2))
            weights.landed(0, 1)

        @pl.when(i == 5)
        def _():
            weights.landed(1, 2)

        @pl.when(i == 6)
        def _():
            weights.landed(1, 1)
        j = i // 2
        gray = j + (j // 2) - 2 * (j // 2) * (j % 2)
        lo, hi = gray % 2, gray // 2
        yhi, ylo = y // 2, y % 2
        yy = 2 * (yhi + hi - 2 * yhi * hi) + (ylo + lo - 2 * ylo * lo)
        flip = i % 2
        zz = zb + flip - 2 * zb * flip
        wait_slot(slot_of(zz, yy, 1 - c))
        compute(zz * 4 + yy)
        return carry

    lax.fori_loop(0, 8, step, 0)

    lam = lam_ref[0, zb]
    gain = jnp.transpose(jnp.broadcast_to(gain_ref[...], (128, 128)))[:, 0:1]
    head = 2 * x + zb

    def head_columns(hh):
        return o_ref.at[:, pl.ds(pl.multiple_of(hh * 128, 128), 128)]

    for qt in (2, 3, 0, 1):
        first, second = acc[qt], acc[per_map + qt]
        combined = first[:128] / first[128:129] - lam * (second[:128] / second[128:129])
        mean_square = jnp.mean(combined * combined, axis=0, keepdims=True)
        value = combined * lax.rsqrt(mean_square + EPSILON) * gain * OUT_SCALE
        att[2 * qt] = jnp.transpose(value[:, :128]).astype(jnp.bfloat16)
        att[2 * qt + 1] = jnp.transpose(value[:, 128:]).astype(jnp.bfloat16)

    sends = []
    for j in range(4):
        xx = (x + j) % 4
        sends.append(pltpu.make_async_remote_copy(
            att.at[4 + xx], head_columns(head), osend.at[j], orecv.at[head],
            device_id={"sp": zpeer, "tp": xx}, device_id_type=MESH))
        sends[-1].start()
    for j in range(1, 4):
        xx = (x + j) % 4
        sends.append(pltpu.make_async_remote_copy(
            att.at[xx], head_columns(head), osend.at[3 + j], orecv.at[head],
            device_id={"sp": s, "tp": xx}, device_id_type=MESH))
        sends[-1].start()
    head_columns(head)[...] = att[x]
    weights.landed(0, 3)
    out_load.wait()
    for j in range(4):
        xx = (x + j) % 4
        for far in range(2):
            if j == 0 and far == 0:
                continue
            hh = 2 * xx + (1 - zb if far else zb)
            pltpu.make_async_remote_copy(
                att.at[0], head_columns(hh), osend.at[0], orecv.at[hh],
                device_id={"sp": zpeer, "tp": x}, device_id_type=MESH).wait_recv()

    square = jnp.zeros((128, 1), jnp.float32)
    for part in range(4):
        here = pl.ds(part * 512, 512)
        mixed = jnp.dot(o_ref[...], wout[:, here], preferred_element_type=jnp.float32).astype(jnp.bfloat16)
        carried = (res_ref[:, here].astype(jnp.float32) + mixed.astype(jnp.float32)).astype(jnp.bfloat16)
        carried_ref[:, here] = carried
        wide = carried.astype(jnp.float32)
        square += jnp.sum(wide * wide, axis=1, keepdims=True)
    level = lax.rsqrt(square * (1.0 / 2048) + EPSILON)
    numbers = lax.broadcasted_iota(jnp.int32, (128, 256), 1)
    pick = jnp.transpose(jnp.where(numbers == place_ref[...], 1.0, 0.0)).astype(jnp.bfloat16)
    for part in range(4):
        here = pl.ds(part * 512, 512)
        normed = (carried_ref[:, here].astype(jnp.float32) * level * ngain_ref[:, here]).astype(jnp.bfloat16)
        tokens = jnp.dot(pick, normed, preferred_element_type=jnp.float32)
        group_ref[:, :, here] = tokens.astype(jnp.bfloat16).reshape(8, 32, 512)
    facts_out[...] = jnp.dot(pick, facts[...], preferred_element_type=jnp.float32).astype(jnp.bfloat16).reshape(8, 32, 128)

    for copy in sends:
        copy.wait_send()
    qcopy.wait_send()
    for own in own_loads:
        pl.when(weights.home)(own.wait)
    weights.finish(0, wg_ref.at[0], (0, 1, 2, 3))
    weights.finish(1, wu_ref.at[0], (0, 1, 2))
    for idx in range(15):
        a, b = pair_copy(own_k, own_v, mine, twin, idx)
        a.wait_send()
        b.wait_send()


def z_of(s):
    return s // 8


def routing(z, ids_ref, rw_ref, facts, place_ref):
    ids = ids_ref[...]
    first, second = ids[:, 0:1], ids[:, 1:2]
    both = jnp.concatenate([jnp.broadcast_to(first, (128, 128)), jnp.broadcast_to(second, (128, 128))], axis=1)
    turned = jnp.transpose(both.astype(jnp.float32)).astype(jnp.int32)
    first_row, second_row = turned[:128], turned[128:]
    earlier = lax.broadcasted_iota(jnp.int32, (128, 128), 1) < lax.broadcasted_iota(jnp.int32, (128, 128), 0)

    def count(mask):
        return jnp.sum(jnp.where(jnp.logical_and(mask, earlier), 1.0, 0.0), axis=1, keepdims=True).astype(jnp.int32)

    slot0 = count(jnp.logical_or(first_row == first, second_row == first))
    slot1 = count(jnp.logical_or(first_row == second, second_row == second))
    group = lax.shift_right_logical(first, 3)
    position = count(lax.shift_right_logical(first_row, 3) == group)
    away = (group - z + 8) & 7
    turn = jnp.where(away == 0, 0, jnp.where(away < 4, 2 * away - 1, 2 * (8 - away)))
    turn = jnp.where(away == 4, 7, turn)
    place_ref[...] = turn * 32 + position
    row0 = ((first & 7) * 16 + slot0).astype(jnp.float32)
    row1 = ((second & 7) * 16 + slot1).astype(jnp.float32)
    w0, w1 = rw_ref[:, 0:1], rw_ref[:, 1:2]
    h0, h1 = w0.astype(jnp.bfloat16).astype(jnp.float32), w1.astype(jnp.bfloat16).astype(jnp.float32)
    lane = lax.broadcasted_iota(jnp.int32, (128, 128), 1)
    table = jnp.zeros((128, 128), jnp.float32)
    for n, column in enumerate((row0, row1, h0, w0 - h0, h1, w1 - h1)):
        table = jnp.where(lane == n, column, table)
    facts[...] = table.astype(jnp.bfloat16)


def attend(queries, keys, values, lambdas, head_gain, w_out, residual_in, norm_gain, route_ids, route_weight, w_gate, w_up):
    rows = queries.shape[0]
    bf, f32 = jnp.bfloat16, jnp.float32
    tiles = 4 * rows // 256
    vm = pl.BlockSpec(memory_space=pltpu.VMEM)
    hbm = pl.BlockSpec(memory_space=pltpu.HBM)
    dma = pltpu.SemaphoreType.DMA
    return pl.pallas_call(
        attend_kernel,
        out_shape=(jax.ShapeDtypeStruct((8, 32, 2048), bf), jax.ShapeDtypeStruct((8, 32, 128), bf),
                   jax.ShapeDtypeStruct((128, 2048), bf), jax.ShapeDtypeStruct((128, 1), jnp.int32),
                   jax.ShapeDtypeStruct((4,) + w_gate.shape[1:], bf), jax.ShapeDtypeStruct((3,) + w_up.shape[1:], bf)),
        in_specs=[pl.BlockSpec(memory_space=pltpu.SMEM), vm, vm, vm, vm, hbm, vm, vm, vm, vm, hbm, hbm],
        out_specs=(vm, vm, vm, vm, vm, vm),
        scratch_shapes=[
            pltpu.VMEM((2, 128, rows), bf),
            pltpu.VMEM((2, 128, rows), bf),
            pltpu.VMEM((8, 2 * rows, 128), bf),
            pltpu.VMEM((16, 144, rows), bf),
            pltpu.VMEM((128, rows), bf),
            pltpu.VMEM((128, 4 * rows), bf),
            pltpu.VMEM((2, 2 * rows, 256), f32),
            pltpu.VMEM((2, 2 * rows, 256), bf),
            pltpu.VMEM((tiles, 144, 256), f32),
            pltpu.VMEM((tiles, 1, 256), f32),
            pltpu.VMEM((8, 128, 128), bf),
            pltpu.VMEM((128, 1024), bf),
            pltpu.VMEM((1024, 2048), bf),
            pltpu.VMEM((128, 128), bf),
            dma((15, 2)), dma((16, 2)), dma((2,)), dma((7,)), dma((8,)), dma((2, 6)), dma((2, 4)), dma((3,)),
        ],
        compiler_params=pltpu.CompilerParams(collective_id=1, has_side_effects=True,
                                             vmem_limit_bytes=48 * 1024 * 1024),
        name="attend",
    )(lambdas.reshape(1, 2), head_gain.reshape(1, 128), queries, keys, values, w_out, residual_in,
      norm_gain.reshape(1, -1), route_ids, route_weight, w_gate, w_up)


Z_STEPS = (0, 1, 7, 2, 6, 3, 5, 4)


def expert_kernel(tok_in, meta_in, place_ref, fg_ref, fu_ref, wd_ref, o_ref,
                  tok, meta, ex, er, ufar, wd, hb, yb, rb, cb, fin,
                  tsend, trecv, msend, mrecv, esend, erecv, ysend, yrecv, fsend, frecv, wsem, dsend, drecv):
    s = lax.axis_index("sp")
    x = lax.axis_index("tp")
    z = s // 8
    y = (s // 2) % 4
    c = s % 2
    side = x // 2
    weights = WeightExchange(s, x, ([None, None, None, ufar], [wd.at[i] for i in range(4)]), dsend, drecv)
    own_down = wd_ref.at[0]

    def z_device(step):
        return ((z + step) % 8) * 8 + y * 2 + c

    def expert_of(k):
        which = k % 2
        stays = 1 - (which + side - 2 * which * side)
        return z * 8 + ((y + k // 2) % 4) * 2 + (1 - stays), stays * x + (1 - stays) * (3 - x)

    def expert_number(k):
        return ((y + k // 2) % 4) * 2 + k % 2

    plane = (1 - c) * x + c * (3 - x)

    def hub_of(h):
        return z * 8 + hub_number(h), plane

    def hub_number(h):
        return ((y + h // 2) % 4) * 2 + (c + h) % 2

    my_expert = y * 2 + side
    other = c == 1

    def self_expert(k):
        return k // 2 == 0

    def when_remote_expert(k, body):
        if k // 2 == 0:
            pl.when(jnp.logical_or(other, side != k % 2))(body)
        else:
            body()

    def when_remote_hub(h, body):
        if h == 0:
            pl.when(other)(body)
        else:
            body()

    barrier = pltpu.get_barrier_semaphore()

    def greet(sp, tp):
        pl.semaphore_signal(barrier, inc=1, device_id={"sp": sp, "tp": tp}, device_id_type=MESH)

    for step in range(1, 8):
        greet(z_device(step), x)
    for k in range(8):
        when_remote_expert(k, lambda k=k: greet(*expert_of(k)))
        when_remote_hub(k, lambda k=k: greet(*hub_of(k)))
    greet(s, weights.beside)
    greet(s, weights.opposite)
    greet(weights.twin, x)
    pl.semaphore_wait(barrier, 24 + 2 * c)

    def token_copies(n):
        dest = {"sp": z_device(Z_STEPS[n]), "tp": x}
        return (pltpu.make_async_remote_copy(tok_in.at[n], tok.at[n], tsend.at[n], trecv.at[n],
                                             device_id=dest, device_id_type=MESH),
                pltpu.make_async_remote_copy(meta_in.at[n], meta.at[n], msend.at[n], mrecv.at[n],
                                             device_id=dest, device_id_type=MESH))

    for n in range(1, 8):
        for copy in token_copies(n):
            copy.start()
    weights.pass_on(0, fu_ref.at[2])
    weights.begin(1, own_down)
    own_load = pltpu.make_async_copy(own_down, wd.at[0], wsem.at[0])
    pl.when(weights.home)(own_load.start)

    tok[0] = tok_in[0]
    meta[0] = meta_in[0]

    row_lanes = lax.broadcasted_iota(jnp.int32, (32, 128), 1).astype(jnp.float32)

    def fact(n, lane):
        return meta[n, :, lane:lane + 1].astype(jnp.float32)

    def chosen(n):
        return row_lanes == fact(n, 0) + 8.0 * (n % 2), row_lanes == fact(n, 1) + 8.0 * (n % 2)

    def spread(n):
        first, second = chosen(n)
        return jnp.transpose(jnp.where(jnp.logical_or(first, second), 1.0, 0.0)).astype(jnp.bfloat16)

    def expert_copy(p, k):
        sp, tp = expert_of(k)
        number = expert_number(k)
        return pltpu.make_async_remote_copy(
            ex.at[p, number], er.at[p, y * 2 + c], esend.at[p, k], erecv.at[p, y * 2 + c],
            device_id={"sp": sp, "tp": tp}, device_id_type=MESH)

    def dispatch(p):
        for n in (2 * p, 2 * p + 1):
            if n > 0:
                for copy in token_copies(n):
                    copy.wait_recv()
        even, odd = spread(2 * p), spread(2 * p + 1)
        for part in range(4):
            here = pl.ds(part * 512, 512)
            block = jnp.dot(even, tok[2 * p, :, here], preferred_element_type=jnp.float32)
            block += jnp.dot(odd, tok[2 * p + 1, :, here], preferred_element_type=jnp.float32)
            ex[p, :, :, here] = block.astype(jnp.bfloat16).reshape(8, 16, 512)
        for k in (0, 1, 2, 3, 6, 7, 4, 5):
            when_remote_expert(k, lambda k=k: expert_copy(p, k).start())

        @pl.when(jnp.logical_not(other))
        def _():
            er[p, y * 2] = ex[p, my_expert]

    def expert_rows_wait(p):
        for h in range(8):
            number = hub_number(h)
            when_remote_hub(h, lambda number=number: pltpu.make_async_remote_copy(
                ex.at[p, 0], er.at[p, number], esend.at[p, 0], erecv.at[p, number],
                device_id={"sp": s, "tp": weights.beside}, device_id_type=MESH).wait_recv())

    def output_copy(p, h):
        sp, tp = hub_of(h)
        return pltpu.make_async_remote_copy(
            yb.at[p, hub_number(h)], rb.at[p, my_expert], ysend.at[p, h], yrecv.at[p, my_expert],
            device_id={"sp": sp, "tp": tp}, device_id_type=MESH)

    def hidden(half):
        def one_quarter(q, carry):
            unit(q, fu_ref[q])
            return carry

        def unit(q, up_weight):
            rows = er[pl.ds(2 * half, 2)].reshape(256, 2048)
            gate = jnp.dot(rows, fg_ref[q], preferred_element_type=jnp.float32)
            up = jnp.dot(rows, up_weight, preferred_element_type=jnp.float32)
            hb[q] = (gate / (1.0 + jnp.exp(-gate)) * up).astype(jnp.bfloat16)

        lax.fori_loop(0, 3, one_quarter, 0)
        if half == 0:
            weights.landed(0, 3)
            weights.finish(0, own_down, (3,))
        unit(3, ufar[...])

    def outputs(half):
        for part in range(8):
            here = pl.ds(part * 256, 256)
            total = None
            for q in range(4):
                term = lax.dot_general(hb[q], wd[q, here, :], (((1,), (1,)), ((), ())),
                                       preferred_element_type=jnp.float32)
                total = term if total is None else total + term
            yb[pl.ds(2 * half, 2), :, :, here] = total.astype(jnp.bfloat16).reshape(2, 8, 16, 256)

    def send_back(p):
        for h in (0, 1, 2, 3, 6, 7, 4, 5):
            when_remote_hub(h, lambda h=h: output_copy(p, h).start())

        @pl.when(jnp.logical_not(other))
        def _():
            rb[p, my_expert] = yb[p, y * 2]

    def final_copy(n):
        dest = {"sp": z_device(8 - Z_STEPS[n]), "tp": x}
        return pltpu.make_async_remote_copy(cb.at[n], fin.at[n], fsend.at[n], frecv.at[n],
                                            device_id=dest, device_id_type=MESH)

    def combine(p):
        for k in range(8):
            number = expert_number(k)
            when_remote_expert(k, lambda number=number: pltpu.make_async_remote_copy(
                yb.at[p, 0], rb.at[p, number], ysend.at[p, 0], yrecv.at[p, number],
                device_id={"sp": s, "tp": weights.beside}, device_id_type=MESH).wait_recv())
        for n in (2 * p, 2 * p + 1):
            first, second = chosen(n)
            high = jnp.where(first, fact(n, 2), 0.0) + jnp.where(second, fact(n, 4), 0.0)
            low = jnp.where(first, fact(n, 3), 0.0) + jnp.where(second, fact(n, 5), 0.0)
            high, low = high.astype(jnp.bfloat16), low.astype(jnp.bfloat16)
            for part in range(4):
                here = pl.ds(part * 512, 512)
                rows = rb[p, :, :, here].reshape(128, 512)
                value = jnp.dot(high, rows, preferred_element_type=jnp.float32)
                value += jnp.dot(low, rows, preferred_element_type=jnp.float32)
                cb[n, :, here] = value.astype(jnp.bfloat16)
            if n > 0:
                final_copy(n).start()

    dispatch(0)
    dispatch(1)
    weights.landed(1, 2)
    weights.pass_on(1)
    dispatch(2)
    expert_rows_wait(0)
    expert_rows_wait(1)
    hidden(0)
    dispatch(3)
    pl.when(weights.home)(own_load.wait)
    weights.landed(1, 1)
    weights.landed(1, 3)
    weights.finish(1, own_down, (0, 1, 2, 3))
    outputs(0)
    send_back(0)
    send_back(1)
    expert_rows_wait(2)
    expert_rows_wait(3)
    hidden(1)
    outputs(1)
    send_back(2)
    send_back(3)
    for p in range(4):
        combine(p)

    for n in range(1, 8):
        final_copy(n).wait_recv()
    fin[0] = cb[0]
    places = lax.broadcasted_iota(jnp.int32, (128, 256), 1)
    pick = jnp.where(places == place_ref[...], 1.0, 0.0).astype(jnp.bfloat16)
    for part in range(4):
        here = pl.ds(part * 512, 512)
        value = jnp.dot(pick, fin[:, :, here].reshape(256, 512), preferred_element_type=jnp.float32)
        o_ref[:, here] = value

    for n in range(1, 8):
        for copy in token_copies(n):
            copy.wait_send()
        final_copy(n).wait_send()
    for p in range(4):
        for k in range(8):
            when_remote_expert(k, lambda k=k: expert_copy(p, k).wait_send())
            when_remote_hub(k, lambda k=k: output_copy(p, k).wait_send())


def experts(grouped, facts, place, full_gate, full_up, w_down):
    bf, f32 = jnp.bfloat16, jnp.float32
    vm = pl.BlockSpec(memory_space=pltpu.VMEM)
    hbm = pl.BlockSpec(memory_space=pltpu.HBM)
    dma = pltpu.SemaphoreType.DMA
    return pl.pallas_call(
        expert_kernel,
        out_shape=jax.ShapeDtypeStruct((128, 2048), f32),
        in_specs=[vm, vm, vm, vm, vm, hbm],
        out_specs=vm,
        scratch_shapes=[
            pltpu.VMEM((8, 32, 2048), bf),
            pltpu.VMEM((8, 32, 128), bf),
            pltpu.VMEM((4, 8, 16, 2048), bf),
            pltpu.VMEM((4, 8, 16, 2048), bf),
            pltpu.VMEM((2048, 256), bf),
            pltpu.VMEM((4, 2048, 256), bf),
            pltpu.VMEM((4, 256, 256), bf),
            pltpu.VMEM((4, 8, 16, 2048), bf),
            pltpu.VMEM((4, 8, 16, 2048), bf),
            pltpu.VMEM((8, 32, 2048), bf),
            pltpu.VMEM((8, 32, 2048), bf),
            dma((8,)), dma((8,)), dma((8,)), dma((8,)),
            dma((4, 8)), dma((4, 8)), dma((4, 8)), dma((4, 8)),
            dma((8,)), dma((8,)), dma((1,)), dma((2, 6)), dma((2, 4)),
        ],
        compiler_params=pltpu.CompilerParams(collective_id=2, has_side_effects=True,
                                             vmem_limit_bytes=46 * 1024 * 1024),
        name="experts",
    )(grouped, facts, place, full_gate, full_up, w_down)


def local(queries, keys, values, lambdas, head_gain, w_out, residual_in, norm_gain,
          route_ids, route_weight, w_gate, w_up, w_down):
    grouped, facts, carried, place, full_gate, full_up = attend(
        queries, keys, values, lambdas, head_gain, w_out, residual_in, norm_gain, route_ids, route_weight, w_gate, w_up)
    mixture = experts(grouped, facts, place, full_gate, full_up, w_down)
    return (carried.astype(jnp.float32) + mixture).astype(jnp.bfloat16)


def solution(mesh):
    placed = (
        P("sp", "tp"), P("sp", "tp"), P("sp", "tp"), P("tp"), P(), P(),
        P(("sp", "tp"), None), P(), P(("sp", "tp"), None), P(("sp", "tp"), None),
        P("sp", None, "tp"), P("sp", None, "tp"), P("sp", None, "tp"),
    )
    return jax.shard_map(local, mesh=mesh, in_specs=placed, out_specs=P(("sp", "tp"), None), check_vma=False)
```

```python
import functools
import jax
import jax.numpy as jnp
from jax import lax
from jax.experimental import pallas as pl
from jax.experimental.pallas import tpu as pltpu
from jax.sharding import PartitionSpec as P

EPSILON = 1e-06
OUT_SCALE = 0.8
FLOOR_SCORE = -1e30
LOG2E = 1.4426950408889634
MESH = pl.DeviceIdType.MESH


class WeightExchange:
    def __init__(self, s, x, places, send, recv):
        self.s, self.x, self.places, self.send, self.recv = s, x, places, send, recv
        self.side = x // 2
        self.home = s % 2 == self.side
        self.away = s % 2 != self.side
        self.beside = x + 1 - 2 * (x % 2)
        self.opposite = 3 - x
        self.twin = s + 1 - 2 * (s % 2)

    def copy(self, m, source, quarter, sp, tp, idx):
        return pltpu.make_async_remote_copy(
            source, self.places[m][quarter], self.send.at[m, idx], self.recv.at[m, quarter],
            device_id={"sp": sp, "tp": tp}, device_id_type=MESH)

    def wait(self, m, quarter):
        self.copy(m, self.places[m][quarter], quarter, self.twin, self.x, 0).wait_recv()

    def share(self, m, quarter, source=None):
        source = self.places[m][quarter] if source is None else source
        self.copy(m, source, quarter, self.twin, self.x, 2 + quarter).start()

    def begin_near(self, m, source):
        @pl.when(self.home)
        def _():
            self.copy(m, source, 1, self.s, self.beside, 0).start()
            self.share(m, 0, source)

    def begin_cross(self, m, source):
        @pl.when(self.away)
        def _():
            self.copy(m, source, 2, self.s, self.opposite, 0).start()

    def pass_on(self, m, block=None):
        @pl.when(self.home)
        def _():
            self.copy(m, self.places[m][2] if block is None else block, 3, self.s, self.beside, 1).start()

    def landed(self, m, quarter):
        @pl.when(self.home)
        def _():
            self.wait(m, quarter)
            self.share(m, quarter)

    def finish(self, m, source, quarters):
        @pl.when(self.home)
        def _():
            if 1 in quarters:
                self.copy(m, source, 1, self.s, self.beside, 0).wait_send()
            if 3 in quarters:
                self.copy(m, source, 3, self.s, self.beside, 1).wait_send()
            for quarter in quarters:
                self.copy(m, source, quarter, self.twin, self.x, 2 + quarter).wait_send()

        @pl.when(self.away)
        def _():
            if 2 in quarters:
                self.copy(m, source, 2, self.s, self.opposite, 0).wait_send()
            for quarter in quarters:
                self.wait(m, quarter)


def attend_kernel(lam_ref, gain_ref, q_in, k_in, v_in, wout_hbm, res_ref, ngain_ref, ids_ref, rw_ref, wg_ref, wu_ref, wd_ref,
                  group_ref, facts_out, carried_ref, place_ref, fg_ref, fu_ref, fd_ref,
                  q_ref, v_ref, kbuf, vbuf, qbuf, qz, sbuf, ebuf, acc, mrun, att, o_ref, wout, facts,
                  ssem, rsem, qsem, osend, orecv, wsend, wrecv, lsem):
    s = lax.axis_index("sp")
    x = lax.axis_index("tp")
    rows = q_in.shape[0]
    zb = (s // 8) % 2
    y = (s // 2) % 4
    c = s % 2
    mine = s % 16
    base = s - mine
    y1 = y + 1 - 2 * (y % 2)
    y3 = 3 - y
    y2 = (y + 2) % 4

    def slot_of(zz, yy, cc):
        return zz * 8 + yy * 2 + cc

    zpeer = base + slot_of(1 - zb, y, c)
    y1dev = base + slot_of(zb, y1, c)
    y3dev = base + slot_of(zb, y3, c)
    twin = base + slot_of(zb, y, 1 - c)

    barrier = pltpu.get_barrier_semaphore()
    peers = [(zpeer, x), (y1dev, x), (y3dev, x), (twin, x)]
    for j in range(1, 4):
        peers.append((s, (x + j) % 4))
        peers.append((zpeer, (x + j) % 4))
    for ps, px in peers:
        pl.semaphore_signal(barrier, inc=1, device_id={"sp": ps, "tp": px}, device_id_type=MESH)
    for b in range(2):
        q_ref[b] = jnp.transpose(q_in[:, 128 * b:128 * (b + 1)])
        v_ref[b] = jnp.transpose(v_in[:, 128 * b:128 * (b + 1)])
    out_load = pltpu.make_async_copy(wout_hbm, wout, lsem.at[0])
    out_load.start()
    pl.semaphore_wait(barrier, len(peers))

    def kslot(slot):
        return kbuf.at[slot // 2, pl.ds(pl.multiple_of((slot % 2) * rows, rows), rows)]

    def vslot(slot):
        return vbuf.at[slot, pl.ds(0, 128)]

    def pair_copy(ksrc, vsrc, slot, dest, idx):
        return (
            pltpu.make_async_remote_copy(ksrc, kslot(slot), ssem.at[idx, 0], rsem.at[slot, 0],
                                         device_id={"sp": dest, "tp": x}, device_id_type=MESH),
            pltpu.make_async_remote_copy(vsrc, vslot(slot), ssem.at[idx, 1], rsem.at[slot, 1],
                                         device_id={"sp": dest, "tp": x}, device_id_type=MESH),
        )

    def start(pair):
        pair[0].start()
        pair[1].start()

    def forward(slot, dest, idx):
        start(pair_copy(kslot(slot), vslot(slot), slot, dest, idx))

    def wait_slot(slot):
        a, b = pair_copy(kslot(slot), vslot(slot), slot, twin, 0)
        a.wait_recv()
        b.wait_recv()

    qcopy = pltpu.make_async_remote_copy(q_ref.at[1 - zb], qbuf, qsem.at[0], qsem.at[1],
                                         device_id={"sp": zpeer, "tp": x}, device_id_type=MESH)
    qcopy.start()

    def key_columns(b):
        return k_in.at[:, pl.ds(pl.multiple_of(b * 128, 128), 128)]

    own_k, own_v = key_columns(zb), v_ref.at[zb]
    start(pair_copy(own_k, own_v, mine, twin, 3))
    start(pair_copy(key_columns(1 - zb), v_ref.at[1 - zb], mine, zpeer, 0))
    start(pair_copy(own_k, own_v, mine, y1dev, 1))
    start(pair_copy(own_k, own_v, mine, y3dev, 2))

    weights = WeightExchange(s, x, ([fg_ref.at[i] for i in range(4)], [fu_ref.at[i] for i in range(3)],
                                    [None, None, fd_ref, None]), wsend, wrecv)
    for m, source in enumerate((wg_ref.at[0], wu_ref.at[0], wd_ref.at[0])):
        weights.begin_cross(m, source)
        if m < 2:
            weights.begin_near(m, source)

    kbuf[mine // 2, pl.ds(pl.multiple_of(c * rows, rows), rows), :] = key_columns(zb)[...]
    vbuf[mine, pl.ds(0, 128), :] = v_ref[zb]
    for slot in range(16):
        vbuf[slot, pl.ds(128, 16), :] = jnp.ones((16, rows), jnp.bfloat16)
    zeros = jnp.zeros((64, rows), jnp.bfloat16)

    def put_queries(value, column):
        qz[pl.ds(0, 64), pl.ds(column, rows)] = value[:64]
        qz[pl.ds(64, 64), pl.ds(column, rows)] = zeros
        qz[pl.ds(0, 64), pl.ds(2 * rows + column, rows)] = zeros
        qz[pl.ds(64, 64), pl.ds(2 * rows + column, rows)] = value[64:]

    put_queries(q_ref[zb], 0)
    mrun[...] = jnp.full(mrun.shape, FLOOR_SCORE, jnp.float32)
    acc[...] = jnp.zeros(acc.shape, jnp.float32)
    routing(z_of(s), ids_ref, rw_ref, facts, place_ref)
    qcopy.wait_recv()
    put_queries(qbuf[...], rows)

    scale = LOG2E * 64 ** (-0.5)
    keys_here = 2 * rows
    tiles = 2 * 2 * rows // 256
    per_map = tiles // 2

    def scores(p, t):
        column = t * 256
        top = None
        for part in range(2):
            value = jnp.dot(kbuf[p, pl.ds(part * rows, rows), :], qz[:, pl.ds(column, 256)],
                            preferred_element_type=jnp.float32)
            sbuf[t % 2, pl.ds(part * rows, rows), :] = value
            peak = jnp.max(value.reshape(rows // 8, 8, 256), axis=0)
            top = peak if top is None else jnp.maximum(top, peak)
        return jnp.max(top, axis=0, keepdims=True) * scale

    def weigh(t, peak):
        old = mrun[t]
        new = jnp.maximum(old, peak)
        mrun[t] = new
        for part in range(4):
            here = pl.ds(part * keys_here // 4, keys_here // 4)
            ebuf[t % 2, here, :] = jnp.exp2(sbuf[t % 2, here, :] * scale - new).astype(jnp.bfloat16)
        return jnp.exp2(old - new)

    def gather_values(p, t, shrink):
        product = jnp.dot(vbuf[2 * p], ebuf[t % 2, pl.ds(0, rows), :], preferred_element_type=jnp.float32)
        product += jnp.dot(vbuf[2 * p + 1], ebuf[t % 2, pl.ds(rows, rows), :], preferred_element_type=jnp.float32)
        acc[t] = acc[t] * shrink + product

    def compute(p):
        peak = scores(p, 0)
        for t in range(tiles):
            following = scores(p, t + 1) if t + 1 < tiles else None
            shrink = weigh(t, peak)
            gather_values(p, t, shrink)
            peak = following

    order = [(0, y), (1, y), (0, y1), (1, y1), (0, y3), (1, y3), (0, y2), (1, y2)]

    def comm(i):
        flip, yy = order[i]
        zz = zb + flip - 2 * zb * flip
        slot = slot_of(zz, yy, c)
        wait_slot(slot)
        if i == 1:
            forward(slot, y1dev, 4)
            forward(slot, y3dev, 5)
        if i == 2:
            forward(slot, y3dev, 8)
        if i == 5:
            forward(slot, y1dev, 12)
        forward(slot, twin, {1: 6, 2: 7, 3: 9, 4: 10, 5: 11, 6: 13, 7: 14}[i])

    def step(i, carry):
        @pl.when(i == 1)
        def _():
            comm(1)
            comm(2)
        for k in range(3, 8):
            @pl.when(i == k - 1)
            def _(k=k):
                comm(k)
        @pl.when(i == 3)
        def _():
            pl.when(weights.home)(lambda: weights.wait(0, 2))
            weights.pass_on(0)
            pl.when(weights.home)(lambda: weights.share(0, 2))
            weights.landed(0, 1)

        @pl.when(i == 5)
        def _():
            weights.landed(1, 2)
            weights.landed(1, 1)
        j = i // 2
        gray = j + (j // 2) - 2 * (j // 2) * (j % 2)
        lo, hi = gray % 2, gray // 2
        yhi, ylo = y // 2, y % 2
        yy = 2 * (yhi + hi - 2 * yhi * hi) + (ylo + lo - 2 * ylo * lo)
        flip = i % 2
        zz = zb + flip - 2 * zb * flip
        wait_slot(slot_of(zz, yy, 1 - c))
        compute(zz * 4 + yy)
        return carry

    lax.fori_loop(0, 8, step, 0)

    lam = lam_ref[0, zb]
    gain = jnp.transpose(jnp.broadcast_to(gain_ref[...], (128, 128)))[:, 0:1]
    head = 2 * x + zb

    def head_columns(hh):
        return o_ref.at[:, pl.ds(pl.multiple_of(hh * 128, 128), 128)]

    for qt in (2, 3, 0, 1):
        first, second = acc[qt], acc[per_map + qt]
        combined = first[:128] / first[128:129] - lam * (second[:128] / second[128:129])
        mean_square = jnp.mean(combined * combined, axis=0, keepdims=True)
        value = combined * lax.rsqrt(mean_square + EPSILON) * gain * OUT_SCALE
        att[2 * qt] = jnp.transpose(value[:, :128]).astype(jnp.bfloat16)
        att[2 * qt + 1] = jnp.transpose(value[:, 128:]).astype(jnp.bfloat16)

    sends = []
    for j in range(4):
        xx = (x + j) % 4
        sends.append(pltpu.make_async_remote_copy(
            att.at[4 + xx], head_columns(head), osend.at[j], orecv.at[head],
            device_id={"sp": zpeer, "tp": xx}, device_id_type=MESH))
        sends[-1].start()
    for j in range(1, 4):
        xx = (x + j) % 4
        sends.append(pltpu.make_async_remote_copy(
            att.at[xx], head_columns(head), osend.at[3 + j], orecv.at[head],
            device_id={"sp": s, "tp": xx}, device_id_type=MESH))
        sends[-1].start()
    head_columns(head)[...] = att[x]
    weights.landed(2, 2)
    weights.landed(0, 3)
    out_load.wait()
    for j in range(4):
        xx = (x + j) % 4
        for far in range(2):
            if j == 0 and far == 0:
                continue
            hh = 2 * xx + (1 - zb if far else zb)
            pltpu.make_async_remote_copy(
                att.at[0], head_columns(hh), osend.at[0], orecv.at[hh],
                device_id={"sp": zpeer, "tp": x}, device_id_type=MESH).wait_recv()

    square = jnp.zeros((128, 1), jnp.float32)
    for part in range(4):
        here = pl.ds(part * 512, 512)
        mixed = jnp.dot(o_ref[...], wout[:, here], preferred_element_type=jnp.float32).astype(jnp.bfloat16)
        carried = (res_ref[:, here].astype(jnp.float32) + mixed.astype(jnp.float32)).astype(jnp.bfloat16)
        carried_ref[:, here] = carried
        wide = carried.astype(jnp.float32)
        square += jnp.sum(wide * wide, axis=1, keepdims=True)
    level = lax.rsqrt(square * (1.0 / 2048) + EPSILON)
    numbers = lax.broadcasted_iota(jnp.int32, (128, 256), 1)
    pick = jnp.transpose(jnp.where(numbers == place_ref[...], 1.0, 0.0)).astype(jnp.bfloat16)
    for part in range(4):
        here = pl.ds(part * 512, 512)
        normed = (carried_ref[:, here].astype(jnp.float32) * level * ngain_ref[:, here]).astype(jnp.bfloat16)
        tokens = jnp.dot(pick, normed, preferred_element_type=jnp.float32)
        group_ref[:, :, here] = tokens.astype(jnp.bfloat16).reshape(8, 32, 512)
    facts_out[...] = jnp.dot(pick, facts[...], preferred_element_type=jnp.float32).astype(jnp.bfloat16).reshape(8, 32, 128)

    for copy in sends:
        copy.wait_send()
    qcopy.wait_send()
    weights.finish(0, wg_ref.at[0], (0, 1, 2, 3))
    weights.finish(1, wu_ref.at[0], (0, 1, 2))
    weights.finish(2, wd_ref.at[0], (2,))
    for idx in range(15):
        a, b = pair_copy(own_k, own_v, mine, twin, idx)
        a.wait_send()
        b.wait_send()


def z_of(s):
    return s // 8


def routing(z, ids_ref, rw_ref, facts, place_ref):
    first_row, second_row = ids_ref[0:1, :], ids_ref[1:2, :]

    def column(row):
        return jnp.transpose(jnp.broadcast_to(row, (128, 128)))[:, 0:1]

    first = column(first_row.astype(jnp.float32)).astype(jnp.int32)
    second = column(second_row.astype(jnp.float32)).astype(jnp.int32)
    earlier = lax.broadcasted_iota(jnp.int32, (128, 128), 1) < lax.broadcasted_iota(jnp.int32, (128, 128), 0)

    def count(mask):
        return jnp.sum(jnp.where(jnp.logical_and(mask, earlier), 1.0, 0.0), axis=1, keepdims=True).astype(jnp.int32)

    slot0 = count(jnp.logical_or(first_row == first, second_row == first))
    slot1 = count(jnp.logical_or(first_row == second, second_row == second))
    group = lax.shift_right_logical(first, 3)
    position = count(lax.shift_right_logical(first_row, 3) == group)
    away = (group - z + 8) & 7
    turn = jnp.where(away == 0, 0, jnp.where(away < 4, 2 * away - 1, 2 * (8 - away)))
    turn = jnp.where(away == 4, 7, turn)
    place_ref[...] = turn * 32 + position
    row0 = ((first & 7) * 16 + slot0).astype(jnp.float32)
    row1 = ((second & 7) * 16 + slot1).astype(jnp.float32)
    w0, w1 = column(rw_ref[0:1, :]), column(rw_ref[1:2, :])
    h0, h1 = w0.astype(jnp.bfloat16).astype(jnp.float32), w1.astype(jnp.bfloat16).astype(jnp.float32)
    lane = lax.broadcasted_iota(jnp.int32, (128, 128), 1)
    table = jnp.zeros((128, 128), jnp.float32)
    for n, value in enumerate((row0, row1, h0, w0 - h0, h1, w1 - h1)):
        table = jnp.where(lane == n, value, table)
    facts[...] = table.astype(jnp.bfloat16)


def attend(queries, keys, values, lambdas, head_gain, w_out, residual_in, norm_gain, route_ids, route_weight, w_gate, w_up, w_down):
    rows = queries.shape[0]
    bf, f32 = jnp.bfloat16, jnp.float32
    tiles = 4 * rows // 256
    vm = pl.BlockSpec(memory_space=pltpu.VMEM)
    hbm = pl.BlockSpec(memory_space=pltpu.HBM)
    dma = pltpu.SemaphoreType.DMA
    return pl.pallas_call(
        attend_kernel,
        out_shape=(jax.ShapeDtypeStruct((8, 32, 2048), bf), jax.ShapeDtypeStruct((8, 32, 128), bf),
                   jax.ShapeDtypeStruct((128, 2048), bf), jax.ShapeDtypeStruct((128, 1), jnp.int32),
                   jax.ShapeDtypeStruct((4,) + w_gate.shape[1:], bf), jax.ShapeDtypeStruct((3,) + w_up.shape[1:], bf),
                   jax.ShapeDtypeStruct(w_down.shape[1:], bf)),
        in_specs=[pl.BlockSpec(memory_space=pltpu.SMEM), vm, vm, vm, vm, hbm, vm, vm, vm, vm, hbm, hbm, hbm],
        out_specs=(vm, vm, vm, vm, hbm, hbm, hbm),
        scratch_shapes=[
            pltpu.VMEM((2, 128, rows), bf),
            pltpu.VMEM((2, 128, rows), bf),
            pltpu.VMEM((8, 2 * rows, 128), bf),
            pltpu.VMEM((16, 144, rows), bf),
            pltpu.VMEM((128, rows), bf),
            pltpu.VMEM((128, 4 * rows), bf),
            pltpu.VMEM((2, 2 * rows, 256), f32),
            pltpu.VMEM((2, 2 * rows, 256), bf),
            pltpu.VMEM((tiles, 144, 256), f32),
            pltpu.VMEM((tiles, 1, 256), f32),
            pltpu.VMEM((8, 128, 128), bf),
            pltpu.VMEM((128, 1024), bf),
            pltpu.VMEM((1024, 2048), bf),
            pltpu.VMEM((128, 128), bf),
            dma((15, 2)), dma((16, 2)), dma((2,)), dma((7,)), dma((8,)), dma((3, 6)), dma((3, 4)), dma((1,)),
        ],
        compiler_params=pltpu.CompilerParams(collective_id=1, has_side_effects=True,
                                             vmem_limit_bytes=63 * 1024 * 1024),
        name="attend",
    )(lambdas.reshape(1, 2), head_gain.reshape(1, 128), queries, keys, values, w_out, residual_in,
      norm_gain.reshape(1, -1), jnp.transpose(route_ids), jnp.transpose(route_weight), w_gate, w_up, w_down)


Z_STEPS = (0, 1, 7, 2, 6, 3, 5, 4)


def expert_kernel(tok_in, meta_in, place_ref, fg_ref, fu_ref, fd_ref, wg_ref, wu_ref, wd_ref, o_ref,
                  tok, meta, ex, er, gw, uw, wd, hb, yb, rb, cb, fin,
                  tsend, trecv, msend, mrecv, esend, erecv, ysend, yrecv, fsend, frecv, wsem, dsend, drecv):
    s = lax.axis_index("sp")
    x = lax.axis_index("tp")
    z = s // 8
    y = (s // 2) % 4
    c = s % 2
    side = x // 2
    weights = WeightExchange(s, x, ([None, None, None, uw.at[3]], [wd.at[i] for i in range(4)]), dsend, drecv)
    own_down = wd_ref.at[0]

    def z_device(step):
        return ((z + step) % 8) * 8 + y * 2 + c

    def expert_of(k):
        which = k % 2
        stays = 1 - (which + side - 2 * which * side)
        return z * 8 + ((y + k // 2) % 4) * 2 + (1 - stays), stays * x + (1 - stays) * (3 - x)

    def expert_number(k):
        return ((y + k // 2) % 4) * 2 + k % 2

    plane = (1 - c) * x + c * (3 - x)

    def hub_of(h):
        return z * 8 + hub_number(h), plane

    def hub_number(h):
        return ((y + h // 2) % 4) * 2 + (c + h) % 2

    my_expert = y * 2 + side
    other = c == 1

    def self_expert(k):
        return k // 2 == 0

    def when_remote_expert(k, body):
        if k // 2 == 0:
            pl.when(jnp.logical_or(other, side != k % 2))(body)
        else:
            body()

    def when_remote_hub(h, body):
        if h == 0:
            pl.when(other)(body)
        else:
            body()

    barrier = pltpu.get_barrier_semaphore()

    def greet(sp, tp):
        pl.semaphore_signal(barrier, inc=1, device_id={"sp": sp, "tp": tp}, device_id_type=MESH)

    for step in range(1, 8):
        greet(z_device(step), x)
    for k in range(8):
        when_remote_expert(k, lambda k=k: greet(*expert_of(k)))
        when_remote_hub(k, lambda k=k: greet(*hub_of(k)))
    greet(s, weights.beside)
    greet(s, weights.opposite)
    greet(weights.twin, x)
    pl.semaphore_wait(barrier, 24 + 2 * c)

    def token_copies(n):
        dest = {"sp": z_device(Z_STEPS[n]), "tp": x}
        return (pltpu.make_async_remote_copy(tok_in.at[n], tok.at[n], tsend.at[n], trecv.at[n],
                                             device_id=dest, device_id_type=MESH),
                pltpu.make_async_remote_copy(meta_in.at[n], meta.at[n], msend.at[n], mrecv.at[n],
                                             device_id=dest, device_id_type=MESH))

    for n in range(1, 8):
        for copy in token_copies(n):
            copy.start()
    weights.pass_on(0, fu_ref.at[2])
    weights.begin_near(1, own_down)
    weights.pass_on(1, fd_ref)
    far_load = pltpu.make_async_copy(fd_ref, wd.at[2], wsem.at[2, 1])
    far_load.start()
    own_load = pltpu.make_async_copy(own_down, wd.at[0], wsem.at[2, 0])

    def load(m, source, q):
        return pltpu.make_async_copy(source, (gw, uw)[m].at[q], wsem.at[m, q])

    full_refs, own_refs = (fg_ref, fu_ref), (wg_ref, wu_ref)

    @pl.when(weights.home)
    def _():
        own_load.start()
        for m in range(2):
            load(m, own_refs[m].at[0], 0).start()

    @pl.when(weights.away)
    def _():
        for m in range(2):
            load(m, full_refs[m].at[0], 0).start()

    later_loads = [load(m, full_refs[m].at[q], q) for q in range(1, 4) for m in range(2) if q < 3 or m == 0]
    for later in later_loads:
        later.start()

    tok[0] = tok_in[0]
    meta[0] = meta_in[0]

    row_lanes = lax.broadcasted_iota(jnp.int32, (32, 128), 1).astype(jnp.float32)

    def fact(n, lane):
        return meta[n, :, lane:lane + 1].astype(jnp.float32)

    def chosen(n):
        return row_lanes == fact(n, 0) + 8.0 * (n % 2), row_lanes == fact(n, 1) + 8.0 * (n % 2)

    def spread(n):
        first, second = chosen(n)
        return jnp.transpose(jnp.where(jnp.logical_or(first, second), 1.0, 0.0)).astype(jnp.bfloat16)

    def expert_copy(p, k):
        sp, tp = expert_of(k)
        number = expert_number(k)
        return pltpu.make_async_remote_copy(
            ex.at[p, number], er.at[p, y * 2 + c], esend.at[p, k], erecv.at[p, y * 2 + c],
            device_id={"sp": sp, "tp": tp}, device_id_type=MESH)

    def dispatch(p):
        for n in (2 * p, 2 * p + 1):
            if n > 0:
                for copy in token_copies(n):
                    copy.wait_recv()
        even, odd = spread(2 * p), spread(2 * p + 1)
        for part in range(4):
            here = pl.ds(part * 512, 512)
            block = jnp.dot(even, tok[2 * p, :, here], preferred_element_type=jnp.float32)
            block += jnp.dot(odd, tok[2 * p + 1, :, here], preferred_element_type=jnp.float32)
            ex[p, :, :, here] = block.astype(jnp.bfloat16).reshape(8, 16, 512)
        for k in (4, 2, 6, 5, 3, 7, 0, 1):
            when_remote_expert(k, lambda k=k: expert_copy(p, k).start())

        @pl.when(jnp.logical_not(other))
        def _():
            er[p, y * 2] = ex[p, my_expert]

    def expert_rows_wait(p):
        for h in range(8):
            number = hub_number(h)
            when_remote_hub(h, lambda number=number: pltpu.make_async_remote_copy(
                ex.at[p, 0], er.at[p, number], esend.at[p, 0], erecv.at[p, number],
                device_id={"sp": s, "tp": weights.beside}, device_id_type=MESH).wait_recv())

    def output_copy(p, h):
        sp, tp = hub_of(h)
        return pltpu.make_async_remote_copy(
            yb.at[p, hub_number(h)], rb.at[p, my_expert], ysend.at[p, h], yrecv.at[p, my_expert],
            device_id={"sp": sp, "tp": tp}, device_id_type=MESH)

    def hidden(p):
        def one_quarter(q, carry):
            rows = er[p].reshape(128, 2048)
            gate = jnp.dot(rows, gw[q], preferred_element_type=jnp.float32)
            up = jnp.dot(rows, uw[q], preferred_element_type=jnp.float32)
            hb[p, q] = (gate / (1.0 + jnp.exp(-gate)) * up).astype(jnp.bfloat16)
            return carry

        expert_rows_wait(p)
        if p == 0:
            for later in later_loads:
                later.wait()
            for m in range(2):
                load(m, full_refs[m].at[0], 0).wait()
            weights.landed(0, 3)
            weights.finish(0, own_down, (3,))
        lax.fori_loop(0, 4, one_quarter, 0)

    def outputs(p):
        def one_part(part, carry):
            here = pl.ds(pl.multiple_of(part * 256, 256), 256)
            total = None
            for q in range(4):
                term = lax.dot_general(hb[p, q], wd[q, here, :], (((1,), (1,)), ((), ())),
                                       preferred_element_type=jnp.float32)
                total = term if total is None else total + term
            yb[p, :, :, here] = total.astype(jnp.bfloat16).reshape(8, 16, 256)
            return carry

        lax.fori_loop(0, 8, one_part, 0)
        send_back(p)

    def send_back(p):
        for h in (4, 2, 6, 5, 3, 7, 0, 1):
            when_remote_hub(h, lambda h=h: output_copy(p, h).start())

        @pl.when(jnp.logical_not(other))
        def _():
            rb[p, my_expert] = yb[p, y * 2]

    def final_copy(n):
        dest = {"sp": z_device(8 - Z_STEPS[n]), "tp": x}
        return pltpu.make_async_remote_copy(cb.at[n], fin.at[n], fsend.at[n], frecv.at[n],
                                            device_id=dest, device_id_type=MESH)

    def combine(p):
        for k in range(8):
            number = expert_number(k)
            when_remote_expert(k, lambda number=number: pltpu.make_async_remote_copy(
                yb.at[p, 0], rb.at[p, number], ysend.at[p, 0], yrecv.at[p, number],
                device_id={"sp": s, "tp": weights.beside}, device_id_type=MESH).wait_recv())
        for n in (2 * p, 2 * p + 1):
            first, second = chosen(n)
            high = jnp.where(first, fact(n, 2), 0.0) + jnp.where(second, fact(n, 4), 0.0)
            low = jnp.where(first, fact(n, 3), 0.0) + jnp.where(second, fact(n, 5), 0.0)
            high, low = high.astype(jnp.bfloat16), low.astype(jnp.bfloat16)
            for part in range(4):
                here = pl.ds(part * 512, 512)
                rows = rb[p, :, :, here].reshape(128, 512)
                value = jnp.dot(high, rows, preferred_element_type=jnp.float32)
                value += jnp.dot(low, rows, preferred_element_type=jnp.float32)
                cb[n, :, here] = value.astype(jnp.bfloat16)
            if n > 0:
                final_copy(n).start()

    dispatch(0)
    dispatch(1)
    hidden(0)
    dispatch(2)
    weights.landed(1, 1)
    hidden(1)
    dispatch(3)
    pl.when(weights.home)(own_load.wait)
    far_load.wait()
    weights.landed(1, 3)
    weights.finish(1, own_down, (0, 1, 3))
    outputs(0)
    outputs(1)
    hidden(2)
    outputs(2)
    combine(0)
    hidden(3)
    outputs(3)
    combine(1)
    combine(2)
    combine(3)

    for n in range(1, 8):
        final_copy(n).wait_recv()
    fin[0] = cb[0]
    places = lax.broadcasted_iota(jnp.int32, (128, 256), 1)
    pick = jnp.where(places == place_ref[...], 1.0, 0.0).astype(jnp.bfloat16)
    for part in range(4):
        here = pl.ds(part * 512, 512)
        value = jnp.dot(pick, fin[:, :, here].reshape(256, 512), preferred_element_type=jnp.float32)
        o_ref[:, here] = value

    for n in range(1, 8):
        for copy in token_copies(n):
            copy.wait_send()
        final_copy(n).wait_send()
    for p in range(4):
        for k in range(8):
            when_remote_expert(k, lambda k=k: expert_copy(p, k).wait_send())
            when_remote_hub(k, lambda k=k: output_copy(p, k).wait_send())


def experts(grouped, facts, place, full_gate, full_up, down_cross, w_gate, w_up, w_down):
    bf, f32 = jnp.bfloat16, jnp.float32
    vm = pl.BlockSpec(memory_space=pltpu.VMEM)
    hbm = pl.BlockSpec(memory_space=pltpu.HBM)
    dma = pltpu.SemaphoreType.DMA
    return pl.pallas_call(
        expert_kernel,
        out_shape=jax.ShapeDtypeStruct((128, 2048), f32),
        in_specs=[vm, vm, vm, hbm, hbm, hbm, hbm, hbm, hbm],
        out_specs=vm,
        scratch_shapes=[
            pltpu.VMEM((8, 32, 2048), bf),
            pltpu.VMEM((8, 32, 128), bf),
            pltpu.VMEM((4, 8, 16, 2048), bf),
            pltpu.VMEM((4, 8, 16, 2048), bf),
            pltpu.VMEM((4, 2048, 256), bf),
            pltpu.VMEM((4, 2048, 256), bf),
            pltpu.VMEM((4, 2048, 256), bf),
            pltpu.VMEM((4, 4, 128, 256), bf),
            pltpu.VMEM((4, 8, 16, 2048), bf),
            pltpu.VMEM((4, 8, 16, 2048), bf),
            pltpu.VMEM((8, 32, 2048), bf),
            pltpu.VMEM((8, 32, 2048), bf),
            dma((8,)), dma((8,)), dma((8,)), dma((8,)),
            dma((4, 8)), dma((4, 8)), dma((4, 8)), dma((4, 8)),
            dma((8,)), dma((8,)), dma((3, 4)), dma((2, 6)), dma((2, 4)),
        ],
        compiler_params=pltpu.CompilerParams(collective_id=2, has_side_effects=True,
                                             vmem_limit_bytes=60 * 1024 * 1024),
        name="experts",
    )(grouped, facts, place, full_gate, full_up, down_cross, w_gate, w_up, w_down)


def local(queries, keys, values, lambdas, head_gain, w_out, residual_in, norm_gain,
          route_ids, route_weight, w_gate, w_up, w_down):
    grouped, facts, carried, place, full_gate, full_up, down_cross = attend(
        queries, keys, values, lambdas, head_gain, w_out, residual_in, norm_gain, route_ids, route_weight,
        w_gate, w_up, w_down)
    mixture = experts(grouped, facts, place, full_gate, full_up, down_cross, w_gate, w_up, w_down)
    return (carried.astype(jnp.float32) + mixture).astype(jnp.bfloat16)


def solution(mesh):
    placed = (
        P("sp", "tp"), P("sp", "tp"), P("sp", "tp"), P("tp"), P(), P(),
        P(("sp", "tp"), None), P(), P(("sp", "tp"), None), P(("sp", "tp"), None),
        P("sp", None, "tp"), P("sp", None, "tp"), P("sp", None, "tp"),
    )
    return jax.shard_map(local, mesh=mesh, in_specs=placed, out_specs=P(("sp", "tp"), None), check_vma=False)
```

```python
import functools
import jax
import jax.numpy as jnp
from jax import lax
from jax.experimental import pallas as pl
from jax.experimental.pallas import tpu as pltpu
from jax.sharding import PartitionSpec as P

EPSILON = 1e-06
OUT_SCALE = 0.8
FLOOR_SCORE = -1e30
LOG2E = 1.4426950408889634
MESH = pl.DeviceIdType.MESH


class WeightExchange:
    def __init__(self, s, x, places, send, recv):
        self.s, self.x, self.places, self.send, self.recv = s, x, places, send, recv
        self.side = x // 2
        self.home = s % 2 == self.side
        self.away = s % 2 != self.side
        self.beside = x + 1 - 2 * (x % 2)
        self.opposite = 3 - x
        self.twin = s + 1 - 2 * (s % 2)

    def copy(self, m, source, quarter, sp, tp, idx):
        return pltpu.make_async_remote_copy(
            source, self.places[m][quarter], self.send.at[m, idx], self.recv.at[m, quarter],
            device_id={"sp": sp, "tp": tp}, device_id_type=MESH)

    def wait(self, m, quarter):
        self.copy(m, self.places[m][quarter], quarter, self.twin, self.x, 0).wait_recv()

    def share(self, m, quarter, source=None):
        source = self.places[m][quarter] if source is None else source
        self.copy(m, source, quarter, self.twin, self.x, 2 + quarter).start()

    def begin_near(self, m, source):
        @pl.when(self.home)
        def _():
            self.copy(m, source, 1, self.s, self.beside, 0).start()
            self.share(m, 0, source)

    def begin_cross(self, m, source):
        @pl.when(self.away)
        def _():
            self.copy(m, source, 2, self.s, self.opposite, 0).start()

    def pass_on(self, m, block=None):
        @pl.when(self.home)
        def _():
            self.copy(m, self.places[m][2] if block is None else block, 3, self.s, self.beside, 1).start()

    def landed(self, m, quarter):
        @pl.when(self.home)
        def _():
            self.wait(m, quarter)
            self.share(m, quarter)

    def finish(self, m, source, quarters):
        @pl.when(self.home)
        def _():
            if 1 in quarters:
                self.copy(m, source, 1, self.s, self.beside, 0).wait_send()
            if 3 in quarters:
                self.copy(m, source, 3, self.s, self.beside, 1).wait_send()
            for quarter in quarters:
                self.copy(m, source, quarter, self.twin, self.x, 2 + quarter).wait_send()

        @pl.when(self.away)
        def _():
            if 2 in quarters:
                self.copy(m, source, 2, self.s, self.opposite, 0).wait_send()
            for quarter in quarters:
                self.wait(m, quarter)


def attend_kernel(lam_ref, gain_ref, q_in, k_in, v_in, wout_hbm, res_ref, ngain_ref, ids_ref, rw_ref, wg_ref, wu_ref, wd_ref,
                  group_ref, facts_out, carried_ref, place_ref, fg_ref, fu_ref, fd_ref,
                  q_ref, v_ref, kbuf, vbuf, qbuf, qz, sbuf, ebuf, acc, mrun, att, o_ref, wout, facts,
                  ssem, rsem, qsem, osend, orecv, wsend, wrecv, lsem):
    s = lax.axis_index("sp")
    x = lax.axis_index("tp")
    rows = q_in.shape[0]
    zb = (s // 8) % 2
    y = (s // 2) % 4
    c = s % 2
    mine = s % 16
    base = s - mine
    y1 = y + 1 - 2 * (y % 2)
    y3 = 3 - y
    y2 = (y + 2) % 4

    def slot_of(zz, yy, cc):
        return zz * 8 + yy * 2 + cc

    zpeer = base + slot_of(1 - zb, y, c)
    y1dev = base + slot_of(zb, y1, c)
    y3dev = base + slot_of(zb, y3, c)
    twin = base + slot_of(zb, y, 1 - c)

    barrier = pltpu.get_barrier_semaphore()
    peers = [(zpeer, x), (y1dev, x), (y3dev, x), (twin, x)]
    for j in range(1, 4):
        peers.append((s, (x + j) % 4))
        peers.append((zpeer, (x + j) % 4))
    for ps, px in peers:
        pl.semaphore_signal(barrier, inc=1, device_id={"sp": ps, "tp": px}, device_id_type=MESH)
    for b in range(2):
        q_ref[b] = jnp.transpose(q_in[:, 128 * b:128 * (b + 1)])
        v_ref[b] = jnp.transpose(v_in[:, 128 * b:128 * (b + 1)])
    out_load = pltpu.make_async_copy(wout_hbm, wout, lsem.at[0])
    out_load.start()
    pl.semaphore_wait(barrier, len(peers))

    def kslot(slot):
        return kbuf.at[slot // 2, pl.ds(pl.multiple_of((slot % 2) * rows, rows), rows)]

    def vslot(slot):
        return vbuf.at[slot, pl.ds(0, 128)]

    def pair_copy(ksrc, vsrc, slot, dest, idx):
        return (
            pltpu.make_async_remote_copy(ksrc, kslot(slot), ssem.at[idx, 0], rsem.at[slot, 0],
                                         device_id={"sp": dest, "tp": x}, device_id_type=MESH),
            pltpu.make_async_remote_copy(vsrc, vslot(slot), ssem.at[idx, 1], rsem.at[slot, 1],
                                         device_id={"sp": dest, "tp": x}, device_id_type=MESH),
        )

    def start(pair):
        pair[0].start()
        pair[1].start()

    def forward(slot, dest, idx):
        start(pair_copy(kslot(slot), vslot(slot), slot, dest, idx))

    def wait_slot(slot):
        a, b = pair_copy(kslot(slot), vslot(slot), slot, twin, 0)
        a.wait_recv()
        b.wait_recv()

    qcopy = pltpu.make_async_remote_copy(q_ref.at[1 - zb], qbuf, qsem.at[0], qsem.at[1],
                                         device_id={"sp": zpeer, "tp": x}, device_id_type=MESH)
    qcopy.start()

    def key_columns(b):
        return k_in.at[:, pl.ds(pl.multiple_of(b * 128, 128), 128)]

    own_k, own_v = key_columns(zb), v_ref.at[zb]
    start(pair_copy(own_k, own_v, mine, twin, 3))
    start(pair_copy(key_columns(1 - zb), v_ref.at[1 - zb], mine, zpeer, 0))
    start(pair_copy(own_k, own_v, mine, y1dev, 1))
    start(pair_copy(own_k, own_v, mine, y3dev, 2))

    weights = WeightExchange(s, x, ([fg_ref.at[i] for i in range(4)], [fu_ref.at[i] for i in range(3)],
                                    [None, None, fd_ref, None]), wsend, wrecv)
    for m, source in enumerate((wg_ref.at[0], wu_ref.at[0], wd_ref.at[0])):
        weights.begin_cross(m, source)
        if m < 2:
            weights.begin_near(m, source)

    kbuf[mine // 2, pl.ds(pl.multiple_of(c * rows, rows), rows), :] = key_columns(zb)[...]
    vbuf[mine, pl.ds(0, 128), :] = v_ref[zb]
    for slot in range(16):
        vbuf[slot, pl.ds(128, 16), :] = jnp.ones((16, rows), jnp.bfloat16)
    zeros = jnp.zeros((64, rows), jnp.bfloat16)

    def put_queries(value, column):
        qz[pl.ds(0, 64), pl.ds(column, rows)] = value[:64]
        qz[pl.ds(64, 64), pl.ds(column, rows)] = zeros
        qz[pl.ds(0, 64), pl.ds(2 * rows + column, rows)] = zeros
        qz[pl.ds(64, 64), pl.ds(2 * rows + column, rows)] = value[64:]

    put_queries(q_ref[zb], 0)
    mrun[...] = jnp.full(mrun.shape, FLOOR_SCORE, jnp.float32)
    acc[...] = jnp.zeros(acc.shape, jnp.float32)
    routing(z_of(s), ids_ref, rw_ref, facts, place_ref)
    qcopy.wait_recv()
    put_queries(qbuf[...], rows)

    scale = LOG2E * 64 ** (-0.5)
    keys_here = 2 * rows
    tiles = 2 * 2 * rows // 256
    per_map = tiles // 2

    def scores(p, t):
        column = t * 256
        top = None
        for part in range(2):
            value = jnp.dot(kbuf[p, pl.ds(part * rows, rows), :], qz[:, pl.ds(column, 256)],
                            preferred_element_type=jnp.float32)
            sbuf[t % 2, pl.ds(part * rows, rows), :] = value
            peak = jnp.max(value.reshape(rows // 8, 8, 256), axis=0)
            top = peak if top is None else jnp.maximum(top, peak)
        return jnp.max(top, axis=0, keepdims=True) * scale

    def weigh(t, peak):
        old = mrun[t]
        new = jnp.maximum(old, peak)
        mrun[t] = new
        for part in range(4):
            here = pl.ds(part * keys_here // 4, keys_here // 4)
            ebuf[t % 2, here, :] = jnp.exp2(sbuf[t % 2, here, :] * scale - new).astype(jnp.bfloat16)
        return jnp.exp2(old - new)

    def gather_values(p, t, shrink):
        product = jnp.dot(vbuf[2 * p], ebuf[t % 2, pl.ds(0, rows), :], preferred_element_type=jnp.float32)
        product += jnp.dot(vbuf[2 * p + 1], ebuf[t % 2, pl.ds(rows, rows), :], preferred_element_type=jnp.float32)
        acc[t] = acc[t] * shrink + product

    def compute(p):
        peak = scores(p, 0)
        for t in range(tiles):
            following = scores(p, t + 1) if t + 1 < tiles else None
            shrink = weigh(t, peak)
            gather_values(p, t, shrink)
            peak = following

    order = [(0, y), (1, y), (0, y1), (1, y1), (0, y3), (1, y3), (0, y2), (1, y2)]

    def comm(i):
        flip, yy = order[i]
        zz = zb + flip - 2 * zb * flip
        slot = slot_of(zz, yy, c)
        there = {1: ((y1dev, 4), (y3dev, 5)), 2: ((y3dev, 8),), 5: ((y1dev, 12),)}.get(i, ())
        there += ((twin, {1: 6, 2: 7, 3: 9, 4: 10, 5: 11, 6: 13, 7: 14}[i]),)
        for half in range(2):
            pair_copy(kslot(slot), vslot(slot), slot, twin, 0)[half].wait_recv()
            for dest, idx in there:
                pair_copy(kslot(slot), vslot(slot), slot, dest, idx)[half].start()

    def step(i, carry):
        @pl.when(i == 1)
        def _():
            comm(1)
            comm(2)
        for k in range(3, 8):
            @pl.when(i == k - 1)
            def _(k=k):
                comm(k)
        @pl.when(i == 3)
        def _():
            pl.when(weights.home)(lambda: weights.wait(0, 2))
            weights.pass_on(0)
            pl.when(weights.home)(lambda: weights.share(0, 2))
            weights.landed(0, 1)

        @pl.when(i == 5)
        def _():
            weights.landed(1, 2)
            weights.landed(1, 1)
        j = i // 2
        gray = j + (j // 2) - 2 * (j // 2) * (j % 2)
        lo, hi = gray % 2, gray // 2
        yhi, ylo = y // 2, y % 2
        yy = 2 * (yhi + hi - 2 * yhi * hi) + (ylo + lo - 2 * ylo * lo)
        flip = i % 2
        zz = zb + flip - 2 * zb * flip
        wait_slot(slot_of(zz, yy, 1 - c))
        compute(zz * 4 + yy)
        return carry

    lax.fori_loop(0, 8, step, 0)

    lam = lam_ref[0, zb]
    gain = jnp.transpose(jnp.broadcast_to(gain_ref[...], (128, 128)))[:, 0:1]
    head = 2 * x + zb

    def head_columns(hh):
        return o_ref.at[:, pl.ds(pl.multiple_of(hh * 128, 128), 128)]

    for qt in (2, 3, 0, 1):
        first, second = acc[qt], acc[per_map + qt]
        combined = first[:128] / first[128:129] - lam * (second[:128] / second[128:129])
        mean_square = jnp.mean(combined * combined, axis=0, keepdims=True)
        value = combined * lax.rsqrt(mean_square + EPSILON) * gain * OUT_SCALE
        att[2 * qt] = jnp.transpose(value[:, :128]).astype(jnp.bfloat16)
        att[2 * qt + 1] = jnp.transpose(value[:, 128:]).astype(jnp.bfloat16)

    sends = []
    for j in range(4):
        xx = (x + j) % 4
        sends.append(pltpu.make_async_remote_copy(
            att.at[4 + xx], head_columns(head), osend.at[j], orecv.at[head],
            device_id={"sp": zpeer, "tp": xx}, device_id_type=MESH))
        sends[-1].start()
    for j in range(1, 4):
        xx = (x + j) % 4
        sends.append(pltpu.make_async_remote_copy(
            att.at[xx], head_columns(head), osend.at[3 + j], orecv.at[head],
            device_id={"sp": s, "tp": xx}, device_id_type=MESH))
        sends[-1].start()
    head_columns(head)[...] = att[x]
    weights.landed(2, 2)
    weights.landed(0, 3)
    out_load.wait()
    for j in range(4):
        xx = (x + j) % 4
        for far in range(2):
            if j == 0 and far == 0:
                continue
            hh = 2 * xx + (1 - zb if far else zb)
            pltpu.make_async_remote_copy(
                att.at[0], head_columns(hh), osend.at[0], orecv.at[hh],
                device_id={"sp": zpeer, "tp": x}, device_id_type=MESH).wait_recv()

    square = jnp.zeros((128, 1), jnp.float32)
    for part in range(4):
        here = pl.ds(part * 512, 512)
        mixed = jnp.dot(o_ref[...], wout[:, here], preferred_element_type=jnp.float32).astype(jnp.bfloat16)
        carried = (res_ref[:, here].astype(jnp.float32) + mixed.astype(jnp.float32)).astype(jnp.bfloat16)
        carried_ref[:, here] = carried
        wide = carried.astype(jnp.float32)
        square += jnp.sum(wide * wide, axis=1, keepdims=True)
    level = lax.rsqrt(square * (1.0 / 2048) + EPSILON)
    numbers = lax.broadcasted_iota(jnp.int32, (128, 256), 1)
    pick = jnp.transpose(jnp.where(numbers == place_ref[...], 1.0, 0.0)).astype(jnp.bfloat16)
    for part in range(4):
        here = pl.ds(part * 512, 512)
        normed = (carried_ref[:, here].astype(jnp.float32) * level * ngain_ref[:, here]).astype(jnp.bfloat16)
        tokens = jnp.dot(pick, normed, preferred_element_type=jnp.float32)
        group_ref[:, :, here] = tokens.astype(jnp.bfloat16).reshape(8, 32, 512)
    facts_out[...] = jnp.dot(pick, facts[...], preferred_element_type=jnp.float32).astype(jnp.bfloat16).reshape(8, 32, 128)

    for copy in sends:
        copy.wait_send()
    qcopy.wait_send()
    weights.finish(0, wg_ref.at[0], (0, 1, 2, 3))
    weights.finish(1, wu_ref.at[0], (0, 1, 2))
    weights.finish(2, wd_ref.at[0], (2,))
    for idx in range(15):
        a, b = pair_copy(own_k, own_v, mine, twin, idx)
        a.wait_send()
        b.wait_send()


def z_of(s):
    return s // 8


def routing(z, ids_ref, rw_ref, facts, place_ref):
    first_row, second_row = ids_ref[0:1, :], ids_ref[1:2, :]

    def column(row):
        return jnp.transpose(jnp.broadcast_to(row, (128, 128)))[:, 0:1]

    first = column(first_row.astype(jnp.float32)).astype(jnp.int32)
    second = column(second_row.astype(jnp.float32)).astype(jnp.int32)
    earlier = lax.broadcasted_iota(jnp.int32, (128, 128), 1) < lax.broadcasted_iota(jnp.int32, (128, 128), 0)

    def count(mask):
        return jnp.sum(jnp.where(jnp.logical_and(mask, earlier), 1.0, 0.0), axis=1, keepdims=True).astype(jnp.int32)

    slot0 = count(jnp.logical_or(first_row == first, second_row == first))
    slot1 = count(jnp.logical_or(first_row == second, second_row == second))
    group = lax.shift_right_logical(first, 3)
    position = count(lax.shift_right_logical(first_row, 3) == group)
    away = (group - z + 8) & 7
    turn = jnp.where(away == 0, 0, jnp.where(away < 4, 2 * away - 1, 2 * (8 - away)))
    turn = jnp.where(away == 4, 7, turn)
    place_ref[...] = turn * 32 + position
    row0 = ((first & 7) * 16 + slot0).astype(jnp.float32)
    row1 = ((second & 7) * 16 + slot1).astype(jnp.float32)
    w0, w1 = column(rw_ref[0:1, :]), column(rw_ref[1:2, :])
    h0, h1 = w0.astype(jnp.bfloat16).astype(jnp.float32), w1.astype(jnp.bfloat16).astype(jnp.float32)
    lane = lax.broadcasted_iota(jnp.int32, (128, 128), 1)
    table = jnp.zeros((128, 128), jnp.float32)
    for n, value in enumerate((row0, row1, h0, w0 - h0, h1, w1 - h1)):
        table = jnp.where(lane == n, value, table)
    facts[...] = table.astype(jnp.bfloat16)


def attend(queries, keys, values, lambdas, head_gain, w_out, residual_in, norm_gain, route_ids, route_weight, w_gate, w_up, w_down):
    rows = queries.shape[0]
    bf, f32 = jnp.bfloat16, jnp.float32
    tiles = 4 * rows // 256
    vm = pl.BlockSpec(memory_space=pltpu.VMEM)
    hbm = pl.BlockSpec(memory_space=pltpu.HBM)
    dma = pltpu.SemaphoreType.DMA
    return pl.pallas_call(
        attend_kernel,
        out_shape=(jax.ShapeDtypeStruct((8, 32, 2048), bf), jax.ShapeDtypeStruct((8, 32, 128), bf),
                   jax.ShapeDtypeStruct((128, 2048), bf), jax.ShapeDtypeStruct((128, 1), jnp.int32),
                   jax.ShapeDtypeStruct((4,) + w_gate.shape[1:], bf), jax.ShapeDtypeStruct((3,) + w_up.shape[1:], bf),
                   jax.ShapeDtypeStruct(w_down.shape[1:], bf)),
        in_specs=[pl.BlockSpec(memory_space=pltpu.SMEM), vm, vm, vm, vm, hbm, vm, vm, vm, vm, hbm, hbm, hbm],
        out_specs=(vm, vm, vm, vm, hbm, hbm, hbm),
        scratch_shapes=[
            pltpu.VMEM((2, 128, rows), bf),
            pltpu.VMEM((2, 128, rows), bf),
            pltpu.VMEM((8, 2 * rows, 128), bf),
            pltpu.VMEM((16, 144, rows), bf),
            pltpu.VMEM((128, rows), bf),
            pltpu.VMEM((128, 4 * rows), bf),
            pltpu.VMEM((2, 2 * rows, 256), f32),
            pltpu.VMEM((2, 2 * rows, 256), bf),
            pltpu.VMEM((tiles, 144, 256), f32),
            pltpu.VMEM((tiles, 1, 256), f32),
            pltpu.VMEM((8, 128, 128), bf),
            pltpu.VMEM((128, 1024), bf),
            pltpu.VMEM((1024, 2048), bf),
            pltpu.VMEM((128, 128), bf),
            dma((15, 2)), dma((16, 2)), dma((2,)), dma((7,)), dma((8,)), dma((3, 6)), dma((3, 4)), dma((1,)),
        ],
        compiler_params=pltpu.CompilerParams(collective_id=1, has_side_effects=True,
                                             vmem_limit_bytes=63 * 1024 * 1024),
        name="attend",
    )(lambdas.reshape(1, 2), head_gain.reshape(1, 128), queries, keys, values, w_out, residual_in,
      norm_gain.reshape(1, -1), jnp.transpose(route_ids), jnp.transpose(route_weight), w_gate, w_up, w_down)


Z_STEPS = (0, 1, 7, 2, 6, 3, 5, 4)


def expert_kernel(tok_in, meta_in, place_ref, fg_ref, fu_ref, fd_ref, wg_ref, wu_ref, wd_ref, o_ref,
                  tok, meta, ex, er, gw, uw, wd, hb, yb, rb, cb, fin,
                  tsend, trecv, msend, mrecv, esend, erecv, ysend, yrecv, fsend, frecv, wsem, dsend, drecv):
    s = lax.axis_index("sp")
    x = lax.axis_index("tp")
    z = s // 8
    y = (s // 2) % 4
    c = s % 2
    side = x // 2
    weights = WeightExchange(s, x, ([None, None, None, uw.at[3]], [wd.at[i] for i in range(4)]), dsend, drecv)
    own_down = wd_ref.at[0]

    def z_device(step):
        return ((z + step) % 8) * 8 + y * 2 + c

    def expert_of(k):
        which = k % 2
        stays = 1 - (which + side - 2 * which * side)
        return z * 8 + ((y + k // 2) % 4) * 2 + (1 - stays), stays * x + (1 - stays) * (3 - x)

    def expert_number(k):
        return ((y + k // 2) % 4) * 2 + k % 2

    plane = (1 - c) * x + c * (3 - x)

    def hub_of(h):
        return z * 8 + hub_number(h), plane

    def hub_number(h):
        return ((y + h // 2) % 4) * 2 + (c + h) % 2

    my_expert = y * 2 + side
    other = c == 1

    def self_expert(k):
        return k // 2 == 0

    def when_remote_expert(k, body):
        if k // 2 == 0:
            pl.when(jnp.logical_or(other, side != k % 2))(body)
        else:
            body()

    def when_remote_hub(h, body):
        if h == 0:
            pl.when(other)(body)
        else:
            body()

    barrier = pltpu.get_barrier_semaphore()

    def greet(sp, tp):
        pl.semaphore_signal(barrier, inc=1, device_id={"sp": sp, "tp": tp}, device_id_type=MESH)

    for step in range(1, 8):
        greet(z_device(step), x)
    for k in range(8):
        when_remote_expert(k, lambda k=k: greet(*expert_of(k)))
        when_remote_hub(k, lambda k=k: greet(*hub_of(k)))
    greet(s, weights.beside)
    greet(s, weights.opposite)
    greet(weights.twin, x)
    pl.semaphore_wait(barrier, 24 + 2 * c)

    def token_copies(n):
        dest = {"sp": z_device(Z_STEPS[n]), "tp": x}
        return (pltpu.make_async_remote_copy(tok_in.at[n], tok.at[n], tsend.at[n], trecv.at[n],
                                             device_id=dest, device_id_type=MESH),
                pltpu.make_async_remote_copy(meta_in.at[n], meta.at[n], msend.at[n], mrecv.at[n],
                                             device_id=dest, device_id_type=MESH))

    for n in (7, 6, 5, 4, 3, 2, 1):
        for copy in token_copies(n):
            copy.start()
    weights.pass_on(0, fu_ref.at[2])
    weights.begin_near(1, own_down)
    weights.pass_on(1, fd_ref)
    far_load = pltpu.make_async_copy(fd_ref, wd.at[2], wsem.at[2, 1])
    far_load.start()
    own_load = pltpu.make_async_copy(own_down, wd.at[0], wsem.at[2, 0])

    def load(m, source, q):
        return pltpu.make_async_copy(source, (gw, uw)[m].at[q], wsem.at[m, q])

    full_refs, own_refs = (fg_ref, fu_ref), (wg_ref, wu_ref)

    @pl.when(weights.home)
    def _():
        own_load.start()
        for m in range(2):
            load(m, own_refs[m].at[0], 0).start()

    @pl.when(weights.away)
    def _():
        for m in range(2):
            load(m, full_refs[m].at[0], 0).start()

    later_loads = [load(m, full_refs[m].at[q], q) for q in range(1, 4) for m in range(2) if q < 3 or m == 0]
    for later in later_loads:
        later.start()

    tok[0] = tok_in[0]
    meta[0] = meta_in[0]

    row_lanes = lax.broadcasted_iota(jnp.int32, (32, 128), 1).astype(jnp.float32)

    def fact(n, lane):
        return meta[n, :, lane:lane + 1].astype(jnp.float32)

    def chosen(n):
        return row_lanes == fact(n, 0) + 8.0 * (n % 2), row_lanes == fact(n, 1) + 8.0 * (n % 2)

    def spread(n):
        first, second = chosen(n)
        return jnp.transpose(jnp.where(jnp.logical_or(first, second), 1.0, 0.0)).astype(jnp.bfloat16)

    def expert_copy(p, k):
        sp, tp = expert_of(k)
        number = expert_number(k)
        return pltpu.make_async_remote_copy(
            ex.at[p, number], er.at[p, y * 2 + c], esend.at[p, k], erecv.at[p, y * 2 + c],
            device_id={"sp": sp, "tp": tp}, device_id_type=MESH)

    def dispatch(p):
        for n in (2 * p, 2 * p + 1):
            if n > 0:
                for copy in token_copies(n):
                    copy.wait_recv()
        even, odd = spread(2 * p), spread(2 * p + 1)
        for part in range(4):
            here = pl.ds(part * 512, 512)
            block = jnp.dot(even, tok[2 * p, :, here], preferred_element_type=jnp.float32)
            block += jnp.dot(odd, tok[2 * p + 1, :, here], preferred_element_type=jnp.float32)
            ex[p, :, :, here] = block.astype(jnp.bfloat16).reshape(8, 16, 512)
        for k in (4, 2, 6, 5, 3, 7, 0, 1):
            when_remote_expert(k, lambda k=k: expert_copy(p, k).start())

        @pl.when(jnp.logical_not(other))
        def _():
            er[p, y * 2] = ex[p, my_expert]

    def expert_rows_wait(p):
        for h in range(8):
            number = hub_number(h)
            when_remote_hub(h, lambda number=number: pltpu.make_async_remote_copy(
                ex.at[p, 0], er.at[p, number], esend.at[p, 0], erecv.at[p, number],
                device_id={"sp": s, "tp": weights.beside}, device_id_type=MESH).wait_recv())

    def output_copy(p, h):
        sp, tp = hub_of(h)
        return pltpu.make_async_remote_copy(
            yb.at[p, hub_number(h)], rb.at[p, my_expert], ysend.at[p, h], yrecv.at[p, my_expert],
            device_id={"sp": sp, "tp": tp}, device_id_type=MESH)

    def hidden(p):
        def one_quarter(q, carry):
            rows = er[p].reshape(128, 2048)
            gate = jnp.dot(rows, gw[q], preferred_element_type=jnp.float32)
            up = jnp.dot(rows, uw[q], preferred_element_type=jnp.float32)
            hb[p, q] = (gate / (1.0 + jnp.exp(-gate)) * up).astype(jnp.bfloat16)
            return carry

        expert_rows_wait(p)
        if p == 3:
            for later in later_loads:
                later.wait()
            for m in range(2):
                load(m, full_refs[m].at[0], 0).wait()
            weights.landed(0, 3)
            weights.finish(0, own_down, (3,))
        lax.fori_loop(0, 4, one_quarter, 0)

    def outputs(p):
        def one_part(part, carry):
            here = pl.ds(pl.multiple_of(part * 256, 256), 256)
            total = None
            for q in range(4):
                term = lax.dot_general(hb[p, q], wd[q, here, :], (((1,), (1,)), ((), ())),
                                       preferred_element_type=jnp.float32)
                total = term if total is None else total + term
            yb[p, :, :, here] = total.astype(jnp.bfloat16).reshape(8, 16, 256)
            return carry

        lax.fori_loop(0, 8, one_part, 0)
        send_back(p)

    def send_back(p):
        for h in (4, 2, 6, 5, 3, 7, 0, 1):
            when_remote_hub(h, lambda h=h: output_copy(p, h).start())

        @pl.when(jnp.logical_not(other))
        def _():
            rb[p, my_expert] = yb[p, y * 2]

    def final_copy(n):
        dest = {"sp": z_device(8 - Z_STEPS[n]), "tp": x}
        return pltpu.make_async_remote_copy(cb.at[n], fin.at[n], fsend.at[n], frecv.at[n],
                                            device_id=dest, device_id_type=MESH)

    def combine(p):
        for k in range(8):
            number = expert_number(k)
            when_remote_expert(k, lambda number=number: pltpu.make_async_remote_copy(
                yb.at[p, 0], rb.at[p, number], ysend.at[p, 0], yrecv.at[p, number],
                device_id={"sp": s, "tp": weights.beside}, device_id_type=MESH).wait_recv())
        for n in (2 * p, 2 * p + 1):
            first, second = chosen(n)
            high = jnp.where(first, fact(n, 2), 0.0) + jnp.where(second, fact(n, 4), 0.0)
            low = jnp.where(first, fact(n, 3), 0.0) + jnp.where(second, fact(n, 5), 0.0)
            high, low = high.astype(jnp.bfloat16), low.astype(jnp.bfloat16)
            for part in range(4):
                here = pl.ds(part * 512, 512)
                rows = rb[p, :, :, here].reshape(128, 512)
                value = jnp.dot(high, rows, preferred_element_type=jnp.float32)
                value += jnp.dot(low, rows, preferred_element_type=jnp.float32)
                cb[n, :, here] = value.astype(jnp.bfloat16)
            if n > 0:
                final_copy(n).start()

    for p in (3, 2, 1, 0):
        dispatch(p)
    hidden(3)
    weights.landed(1, 1)
    hidden(2)
    pl.when(weights.home)(own_load.wait)
    far_load.wait()
    weights.landed(1, 3)
    weights.finish(1, own_down, (0, 1, 3))
    outputs(3)
    outputs(2)
    hidden(1)
    outputs(1)
    combine(3)
    hidden(0)
    outputs(0)
    combine(2)
    combine(1)
    combine(0)

    for n in range(1, 8):
        final_copy(n).wait_recv()
    fin[0] = cb[0]
    places = lax.broadcasted_iota(jnp.int32, (128, 256), 1)
    pick = jnp.where(places == place_ref[...], 1.0, 0.0).astype(jnp.bfloat16)
    for part in range(4):
        here = pl.ds(part * 512, 512)
        value = jnp.dot(pick, fin[:, :, here].reshape(256, 512), preferred_element_type=jnp.float32)
        o_ref[:, here] = value

    for n in range(1, 8):
        for copy in token_copies(n):
            copy.wait_send()
        final_copy(n).wait_send()
    for p in range(4):
        for k in range(8):
            when_remote_expert(k, lambda k=k: expert_copy(p, k).wait_send())
            when_remote_hub(k, lambda k=k: output_copy(p, k).wait_send())


def experts(grouped, facts, place, full_gate, full_up, down_cross, w_gate, w_up, w_down):
    bf, f32 = jnp.bfloat16, jnp.float32
    vm = pl.BlockSpec(memory_space=pltpu.VMEM)
    hbm = pl.BlockSpec(memory_space=pltpu.HBM)
    dma = pltpu.SemaphoreType.DMA
    return pl.pallas_call(
        expert_kernel,
        out_shape=jax.ShapeDtypeStruct((128, 2048), f32),
        in_specs=[vm, vm, vm, hbm, hbm, hbm, hbm, hbm, hbm],
        out_specs=vm,
        scratch_shapes=[
            pltpu.VMEM((8, 32, 2048), bf),
            pltpu.VMEM((8, 32, 128), bf),
            pltpu.VMEM((4, 8, 16, 2048), bf),
            pltpu.VMEM((4, 8, 16, 2048), bf),
            pltpu.VMEM((4, 2048, 256), bf),
            pltpu.VMEM((4, 2048, 256), bf),
            pltpu.VMEM((4, 2048, 256), bf),
            pltpu.VMEM((4, 4, 128, 256), bf),
            pltpu.VMEM((4, 8, 16, 2048), bf),
            pltpu.VMEM((4, 8, 16, 2048), bf),
            pltpu.VMEM((8, 32, 2048), bf),
            pltpu.VMEM((8, 32, 2048), bf),
            dma((8,)), dma((8,)), dma((8,)), dma((8,)),
            dma((4, 8)), dma((4, 8)), dma((4, 8)), dma((4, 8)),
            dma((8,)), dma((8,)), dma((3, 4)), dma((2, 6)), dma((2, 4)),
        ],
        compiler_params=pltpu.CompilerParams(collective_id=2, has_side_effects=True,
                                             vmem_limit_bytes=60 * 1024 * 1024),
        name="experts",
    )(grouped, facts, place, full_gate, full_up, down_cross, w_gate, w_up, w_down)


def local(queries, keys, values, lambdas, head_gain, w_out, residual_in, norm_gain,
          route_ids, route_weight, w_gate, w_up, w_down):
    grouped, facts, carried, place, full_gate, full_up, down_cross = attend(
        queries, keys, values, lambdas, head_gain, w_out, residual_in, norm_gain, route_ids, route_weight,
        w_gate, w_up, w_down)
    mixture = experts(grouped, facts, place, full_gate, full_up, down_cross, w_gate, w_up, w_down)
    return (carried.astype(jnp.float32) + mixture).astype(jnp.bfloat16)


def solution(mesh):
    placed = (
        P("sp", "tp"), P("sp", "tp"), P("sp", "tp"), P("tp"), P(), P(),
        P(("sp", "tp"), None), P(), P(("sp", "tp"), None), P(("sp", "tp"), None),
        P("sp", None, "tp"), P("sp", None, "tp"), P("sp", None, "tp"),
    )
    return jax.shard_map(local, mesh=mesh, in_specs=placed, out_specs=P(("sp", "tp"), None), check_vma=False)
```
